128 devices in a mesh: sp: 16 (over z, y), fs: 4 (over x), tp: 2 (over core).
Axes of the slice: x: 4, y: 4, z: 4, core: 2. Of those that a mesh axis runs over, the one named last changes fastest.
Arguments:
- hidden_in: bfloat16 [32768, 2048], P(('fs', 'sp'), 'tp'), parts along dimension 0, may hold values from -6 to 48
- in_gain: float32 [2048], replicated, may hold values from 0.1 to 1.9
- w_query: bfloat16 [2048, 1024], P(None, 'tp'), may hold values from -0.29972302 to 0.29972302
- w_key: bfloat16 [2048, 1024], P(None, 'tp'), may hold values from -0.29972302 to 0.29972302
- w_value: bfloat16 [2048, 1024], P(None, 'tp'), may hold values from -0.125 to 0.125
- w_gate: bfloat16 [2048, 1024], P(None, 'tp'), may hold values from -0.125 to 0.125
- w_inner: bfloat16 [2048, 1024], P(None, 'tp'), may hold values from -0.125 to 0.125
- w_bvec: bfloat16 [2048, 512], P(None, 'tp'), may hold values from -0.125 to 0.125
- w_cvec: bfloat16 [2048, 512], P(None, 'tp'), may hold values from -0.125 to 0.125
- w_step: bfloat16 [2048, 16], P(None, 'tp'), may hold values from -0.125 to 0.125
- conv_inner: bfloat16 [4, 1024], P(None, 'tp'), may hold values from -3 to 3
- conv_bvec: bfloat16 [4, 512], P(None, 'tp'), may hold values from -3 to 3
- conv_cvec: bfloat16 [4, 512], P(None, 'tp'), may hold values from -3 to 3
- a_log: float32 [16], P('tp'), may hold values from -16 to 0
- decay_add: float32 [32768, 16], P(('fs', 'sp'), 'tp'), parts along dimension 0, may hold values from -1 to 0
- lambdas: float32 [4], P('tp'), may hold values from 0.3 to 0.8
- head_gain: float32 [256], replicated, may hold values from 0.1 to 1.9
- ssm_gain: float32 [1024], P('tp'), may hold values from 0.1 to 1.9
- out_attn: bfloat16 [1024, 2048], P('tp'), may hold values from -0.125 to 0.125
- out_ssm: bfloat16 [1024, 2048], P('tp'), may hold values from -0.125 to 0.125
Outputs:
- layer_out: bfloat16 [32768, 2048], P(('fs', 'sp', 'tp')), parts along dimension 0
The draws below stay inside these ranges and needn't reach their ends.
There are 4 independent parts, one for each index of `fs`. The reference program is written for one: setup_inputs(seed, part) draws one part's arguments, and reference() takes and returns one part's arrays. A program takes and returns all parts, laid end to end along the dimension named above; an argument that names none is the same for every part. Nothing has to cross between parts.
All inputs are finite; a program needn't handle non-finite values.
Results may differ from the reference program's by a relative error of at most 0.012.
The reference program's roundings to bfloat16 on the way (of `normed`, `attn_out` and `ssm_out`) count: a program that leaves them out, or rounds other values in their place, can miss the bound.
Values may be sent and summed in bfloat16 or wider, within the bound.
A program may use at most 128 MiB of HBM per device.

```python
import math
import jax
import jax.numpy as jnp
from jax import lax

D = 2048
ATTN_HEADS = 4
QK_DIM = 128
MIXER_HEADS = 16
SSM_P = 64
STATE = 128
GROUPS = 4
CONV_TAPS = 4
BLOCK = 128
SEQUENCE_LENGTH = 8192
ATTN_W = 1024
SSM_W = 1024
BC = 512


def drawn_columns(key):
    shared = jax.random.fold_in(key, 11)
    spread = 1.6 * (D * 10 // 17) ** (-0.5)
    return jax.random.truncated_normal(shared, -4.0, 4.0, (ATTN_W,), jnp.float32) * spread


def drawn_weight(key, salt):
    own_key = jax.random.fold_in(key, salt)
    spread = (D * 10 // 17) ** (-0.5)
    base = jax.random.truncated_normal(own_key, -4.0, 4.0, (D, ATTN_W), jnp.float32) * spread
    leading = (jnp.arange(D) < 8).astype(jnp.float32)[:, None]
    return base + leading * drawn_columns(key)[None, :]


def draw_w_query(key, part):
    return drawn_weight(key, 1).astype(jnp.bfloat16)


def draw_w_key(key, part):
    return drawn_weight(key, 2).astype(jnp.bfloat16)


def draw_hidden_in(key, part):
    base_key = jax.random.fold_in(key, 21)
    position_random_key = jax.random.fold_in(key, 22)
    size_key = jax.random.fold_in(key, 23)
    count = max(4, SEQUENCE_LENGTH // 512)
    base = jax.random.truncated_normal(base_key, -6.0, 6.0, (SEQUENCE_LENGTH, D), jnp.float32)
    strength = jax.random.uniform(size_key, (count,), jnp.float32, 8.0, 32.0)
    places = jax.random.randint(position_random_key, (count,), 0, SEQUENCE_LENGTH)
    hits = jnp.arange(SEQUENCE_LENGTH)[:, None] == places[None, :]
    level = jnp.max(jnp.where(hits, strength[None, :], 0.0), axis=1)
    planted = (level > 0.0)[:, None] & (jnp.arange(D) < 8)[None, :]
    return jnp.where(planted, level[:, None], base).astype(jnp.bfloat16)


def draw_a_log(key, part):
    order_key, slow_key, fast_key = jax.random.split(key, 3)
    head_order = jax.random.permutation(order_key, MIXER_HEADS)
    fast_heads = head_order < MIXER_HEADS // 2
    slow_rate = jax.random.uniform(slow_key, (MIXER_HEADS,), jnp.float32, 0.1, 0.4) / SEQUENCE_LENGTH
    fast_rate = jax.random.uniform(fast_key, (MIXER_HEADS,), jnp.float32, 0.015, 0.04)
    return jnp.log(jnp.where(fast_heads, fast_rate, slow_rate))


def draw_decay_add(key, part):
    rate_key, rough_key, position_random_key, depth_random_key = jax.random.split(key, 4)
    block_count = SEQUENCE_LENGTH // BLOCK
    block_rates = jnp.exp(jax.random.uniform(rate_key, (block_count, 1), jnp.float32, jnp.log(0.15), jnp.log(1.2))) / SEQUENCE_LENGTH
    roughness = jax.random.uniform(rough_key, (SEQUENCE_LENGTH, MIXER_HEADS), jnp.float32, 0.5, 1.5)
    steady_baseline = -jnp.repeat(block_rates, BLOCK, axis=0) * roughness
    spike_positions = jax.random.randint(position_random_key, (3,), 0, SEQUENCE_LENGTH)
    spike_depth = jnp.log(jax.random.uniform(depth_random_key, (3, MIXER_HEADS), jnp.float32, 0.5, 0.8))
    spike_rows = (jnp.arange(SEQUENCE_LENGTH)[:, None] == spike_positions[None, :]).astype(jnp.float32)
    return steady_baseline + jnp.dot(spike_rows, spike_depth, precision=jax.lax.Precision.HIGHEST)


def level_of(rng, extent, cuts, low, largest):
    loudness = 1.0
    for axis_at, shards_of in cuts:
        heights = jax.random.uniform(jax.random.fold_in(jax.random.fold_in(rng, 6), axis_at), (shards_of,), jnp.float32, low / len(cuts), largest / len(cuts))
        loudness = loudness * jnp.repeat(jnp.exp(heights), extent[axis_at] // shards_of).reshape((-1,) + (1,) * (len(extent) - 1 - axis_at))
    return loudness


def noise(key, extent, scale, most, cuts=(), held_as=jnp.bfloat16):
    entries = scale * jax.random.normal(key, extent, jnp.float32)
    if cuts:
        entries = entries * level_of(key, extent, cuts, -0.22, 0.18)
    return jnp.clip(entries, -most, most).astype(held_as)


def setup_inputs(seed: int = 0, part: int = 0) -> dict:
    streams_of = jax.random.split(jax.random.key(seed), 21)
    part_keys = jax.random.split(jax.random.fold_in(streams_of[20], part), 21)
    return {
        "hidden_in": draw_hidden_in(jax.random.fold_in(jax.random.fold_in(streams_of[20], part), 71), part),
        "in_gain": jnp.clip(1.0 + 0.18 * jax.random.normal(streams_of[1], (D,), jnp.float32), 0.1, 1.9),
        "w_query": draw_w_query(jax.random.fold_in(streams_of[20], 71), part),
        "w_key": draw_w_key(jax.random.fold_in(streams_of[20], 71), part),
        "w_value": noise(streams_of[4], (D, ATTN_W), D ** -0.5, 0.125, ((1, 2),)),
        "w_gate": noise(streams_of[5], (D, SSM_W), D ** -0.5, 0.125, ((1, 2),)),
        "w_inner": noise(streams_of[6], (D, SSM_W), D ** -0.5, 0.125, ((1, 2),)),
        "w_bvec": noise(streams_of[7], (D, BC), D ** -0.5, 0.125, ((1, 2),)),
        "w_cvec": noise(streams_of[8], (D, BC), D ** -0.5, 0.125, ((1, 2),)),
        "w_step": noise(streams_of[9], (D, MIXER_HEADS), D ** -0.5, 0.125, ((1, 2),)),
        "conv_inner": noise(streams_of[10], (CONV_TAPS, SSM_W), 0.5, 3.0, ((1, 2),)),
        "conv_bvec": noise(streams_of[11], (CONV_TAPS, BC), 0.5, 3.0, ((1, 2),)),
        "conv_cvec": noise(streams_of[12], (CONV_TAPS, BC), 0.5, 3.0, ((1, 2),)),
        "a_log": draw_a_log(jax.random.fold_in(streams_of[20], 71), part),
        "decay_add": draw_decay_add(jax.random.fold_in(jax.random.fold_in(streams_of[20], part), 71), part),
        "lambdas": jnp.clip(0.3 + 0.5 * jax.random.uniform(streams_of[15], (ATTN_HEADS,), jnp.float32) ** level_of(streams_of[15], (ATTN_HEADS,), ((0, 2),), -0.2, 0.2), 0.3, 0.8),
        "head_gain": jnp.clip(1.0 + 0.18 * jax.random.normal(streams_of[16], (2 * QK_DIM,), jnp.float32), 0.1, 1.9),
        "ssm_gain": jnp.clip(1.0 + 0.18 * jax.random.normal(streams_of[17], (SSM_W,), jnp.float32), 0.1, 1.9),
        "out_attn": noise(streams_of[18], (ATTN_W, D), (ATTN_W + SSM_W) ** -0.5, 0.125, ((0, 2),)),
        "out_ssm": noise(streams_of[19], (SSM_W, D), (ATTN_W + SSM_W) ** -0.5, 0.125, ((0, 2),)),
    }


EPS = 1e-06
NEG = -1e+30

def rms_rows(values, gain):
    return values * lax.rsqrt(lax.optimization_barrier(jnp.mean(values * values, axis=-1, keepdims=True)) + EPS) * gain

def stored(values):
    return lax.optimization_barrier(values.astype(jnp.bfloat16))

def reference(hidden_in, in_gain, w_query, w_key, w_value, w_gate, w_inner, w_bvec, w_cvec, w_step, conv_inner, conv_bvec, conv_cvec, a_log, decay_add, lambdas, head_gain, ssm_gain, out_attn, out_ssm):
    length = hidden_in.shape[0]
    normed = stored(rms_rows(hidden_in.astype(jnp.float32), in_gain))

    def project(weight):
        return stored(jnp.dot(normed, weight, preferred_element_type=jnp.float32))
    query = project(w_query).reshape(length, ATTN_HEADS, 2, QK_DIM)
    keys = project(w_key).reshape(length, ATTN_HEADS, 2, QK_DIM).astype(jnp.float32)
    values = project(w_value).reshape(length, ATTN_HEADS, 2 * QK_DIM).astype(jnp.float32)
    gate_z = project(w_gate)
    inner = project(w_inner)
    b_pre = project(w_bvec)
    c_pre = project(w_cvec)
    step_pre = project(w_step)
    scale = QK_DIM ** (-0.5)
    positions = jnp.arange(length).astype(jnp.int32)
    row_block = math.gcd(length, 512)

    def attend(start):
        query_rows = lax.dynamic_slice_in_dim(query, start, row_block, 0).astype(jnp.float32)
        scores = jnp.einsum('qhmd,khmd->qhmk', query_rows, keys) * scale
        query_pos = start + jnp.arange(row_block).astype(jnp.int32)
        visible = (positions[None, :] <= query_pos[:, None])[:, None, None, :]
        peak = lax.optimization_barrier(jnp.max(jnp.where(visible, scores, NEG), axis=-1, keepdims=True))
        weights = jnp.where(visible, jnp.exp(scores - peak), 0.0)
        totals = lax.optimization_barrier(jnp.sum(weights, axis=-1))
        mixed = jnp.einsum('qhmk,khe->qhme', stored(weights).astype(jnp.float32), values)
        first_map = mixed[:, :, 0] / totals[:, :, 0, None]
        second_map = mixed[:, :, 1] / totals[:, :, 1, None]
        differ = first_map - lambdas[None, :, None] * second_map
        return stored(rms_rows(differ, head_gain)).reshape(row_block, ATTN_W)
    starts = jnp.arange(0, length, row_block).astype(jnp.int32)
    attn_out = lax.map(attend, starts).reshape(length, ATTN_W)

    def convolve(pre, weight):
        padded = jnp.pad(pre.astype(jnp.float32), ((CONV_TAPS - 1, 0), (0, 0)))
        summed = padded[0:length] * weight[0].astype(jnp.float32)
        for offset in range(1, CONV_TAPS):
            summed = summed + padded[offset:offset + length] * weight[offset].astype(jnp.float32)
        return stored(jax.nn.silu(summed))
    per_group = MIXER_HEADS // GROUPS
    block_count = length // BLOCK
    inputs_x = convolve(inner, conv_inner).reshape(block_count, BLOCK, MIXER_HEADS, SSM_P)
    inputs_b = convolve(b_pre, conv_bvec).reshape(block_count, BLOCK, GROUPS, STATE)
    inputs_c = convolve(c_pre, conv_cvec).reshape(block_count, BLOCK, GROUPS, STATE)
    step_size = jax.nn.softplus(step_pre.astype(jnp.float32))
    log_decay = -jnp.exp(a_log)[None, :] * step_size + decay_add
    causal = jnp.tril(jnp.ones((BLOCK, BLOCK), dtype=bool))

    def block_step(state, items):
        block_x, block_b, block_c, block_size, block_decay = items
        running = jnp.cumsum(block_decay, axis=0)
        decay = jnp.exp(jnp.where(causal[:, :, None], running[:, None, :] - running[None, :, :], NEG))
        intersection = jnp.einsum('tgk,sgk->tsg', block_c.astype(jnp.float32), block_b.astype(jnp.float32))
        matrix = stored(jnp.repeat(intersection, per_group, axis=2) * decay * block_size[None, :, :])
        inside = jnp.einsum('tsh,shp->thp', matrix.astype(jnp.float32), block_x.astype(jnp.float32))
        heads_c = jnp.repeat(block_c, per_group, axis=1).astype(jnp.float32)
        carried = jnp.einsum('thk,hpk->thp', heads_c, state, precision=lax.Precision.HIGHEST) * jnp.exp(running)[:, :, None]
        to_end = jnp.exp(running[-1:] - running) * block_size
        weighted = stored(block_x.astype(jnp.float32) * to_end[:, :, None])
        heads_b = jnp.repeat(block_b, per_group, axis=1).astype(jnp.float32)
        fresh = jnp.einsum('shp,shk->hpk', weighted.astype(jnp.float32), heads_b)
        return (state * jnp.exp(running[-1])[:, None, None] + fresh, inside + carried)
    start_state = jnp.zeros((MIXER_HEADS, SSM_P, STATE), jnp.float32)
    items = (inputs_x, inputs_b, inputs_c, step_size.reshape(block_count, BLOCK, MIXER_HEADS), log_decay.reshape(block_count, BLOCK, MIXER_HEADS))
    final_state, outputs = lax.scan(block_step, start_state, items)
    gated = outputs.reshape(length, SSM_W) * jax.nn.silu(gate_z.astype(jnp.float32))
    grouped = rms_rows(gated.reshape(length, GROUPS, SSM_W // GROUPS), 1.0)
    ssm_out = stored(grouped.reshape(length, SSM_W) * ssm_gain)
    joined = jnp.dot(attn_out, out_attn, preferred_element_type=jnp.float32) + jnp.dot(ssm_out, out_ssm, preferred_element_type=jnp.float32)
    return joined.astype(jnp.bfloat16)
```

```python
import jax
import jax.numpy as jnp
from jax import lax
from jax.experimental import pallas as pl
from jax.experimental.pallas import tpu as pltpu
from jax.sharding import Mesh
from jax.sharding import PartitionSpec as P

D = 2048
QK_DIM = 128
SSM_P = 64
STATE = 128
BLOCK = 128
KEY_BLOCK = 128
SP = ("sp_0", "sp_1")
FS_SP = ("fs", "sp_0", "sp_1")
FS_SP_TP = ("fs", "sp_0", "sp_1", "tp")


EPS = 1e-06
NEG = -1e30


HALF = 256
PAIR = 256
MESH = pl.DeviceIdType.MESH
ORDER = (0, 1, 3, 2)
SCALE2 = QK_DIM ** (-0.5) * 1.4426950408889634


def attention_kernel(
    kv_in,
    q_in,
    lam_ref,
    gain_ref,
    out_ref,
    kv,
    q,
    acc,
    peak,
    total,
    done_out,
    back,
    zs_send,
    zs_recv,
    zq_send,
    zq_recv,
    ring_send,
    kv_recv,
    core_send,
    back_send,
    back_recv,
):
    z, y, c = lax.axis_index("sp_0"), lax.axis_index("sp_1"), lax.axis_index("tp")
    right, left = lax.rem(y + 1, 4), lax.rem(y + 3, 4)
    other = 1 - c
    barrier = pltpu.get_barrier_semaphore()
    for dz in range(4):
        zz = lax.rem(z + dz, 4)
        for dc in range(2):
            if dz or dc:
                pl.semaphore_signal(
                    barrier,
                    inc=1,
                    device_id={"sp_0": zz, "tp": lax.rem(c + dc, 2)},
                    device_id_type=MESH,
                )
    for yy in (left, right):
        pl.semaphore_signal(barrier, inc=1, device_id={"sp_1": yy}, device_id_type=MESH)
    pl.semaphore_wait(barrier, 9)

    def exchange(src, dst_of, send, recv, j):
        i, r = j // 2, j % 2
        to = 2 * c + i
        mine = jnp.logical_and(to == z, c == r)

        @pl.when(mine)
        def _():
            pltpu.make_async_copy(src.at[j], dst_of(z), recv.at[z]).start()

        @pl.when(jnp.logical_not(mine))
        def _():
            pltpu.make_async_remote_copy(
                src_ref=src.at[j],
                dst_ref=dst_of(z),
                send_sem=send.at[j],
                recv_sem=recv.at[z],
                device_id={"sp_0": to, "tp": r},
                device_id_type=MESH,
            ).start()

    for j in range(4):
        exchange(kv_in, lambda zz: kv.at[0, zz], zs_send, zs_recv, j)
    for j in range(4):
        exchange(q_in, lambda zz: q.at[zz], zq_send, zq_recv, j)

    acc[...] = jnp.zeros_like(acc)
    total[...] = jnp.zeros_like(total)
    peak[...] = jnp.full_like(peak, NEG)

    def arrived(ref, sem):
        pltpu.make_async_copy(ref, ref, sem).wait()

    def to_neighbour(slot, zz, new_slot, yy, k):
        return pltpu.make_async_remote_copy(
            src_ref=kv.at[slot, zz],
            dst_ref=kv.at[new_slot, zz],
            send_sem=ring_send.at[k],
            recv_sem=kv_recv.at[new_slot, zz],
            device_id={"sp_1": yy},
            device_id_type=MESH,
        )

    def to_partner(slot, zz):
        return pltpu.make_async_remote_copy(
            src_ref=kv.at[slot, zz],
            dst_ref=kv.at[slot + 1, zz],
            send_sem=core_send.at[slot // 2, zz],
            recv_sem=kv_recv.at[slot + 1, zz],
            device_id={"tp": other},
            device_id_type=MESH,
        )

    def wait_chunk(slot, zz):
        arrived(kv.at[slot, zz], kv_recv.at[slot, zz])

    own = 2 * y + c

    def block(zq, slot, zc, masked):
        for m in range(2):
            lanes = slice(m * QK_DIM, (m + 1) * QK_DIM)
            scores = (
                jnp.dot(
                    kv[slot, zc, 0, :, lanes], q[zq, lanes, :], preferred_element_type=jnp.float32
                )
                * SCALE2
            )
            if masked:
                key_at = lax.broadcasted_iota(jnp.int32, scores.shape, 0)
                query_at = lax.broadcasted_iota(jnp.int32, scores.shape, 1)
                scores = jnp.where(key_at <= query_at, scores, NEG)
            old = peak[zq, m]
            new = jnp.maximum(old, jnp.max(scores, axis=0, keepdims=True))
            weights = jnp.exp2(scores - new[0:1])
            shrink = jnp.exp2(old - new)
            peak[zq, m] = new
            total[zq, m] = total[zq, m] * shrink + jnp.sum(weights, axis=0, keepdims=True)
            acc[zq, m] = acc[zq, m] * shrink[0:1] + jnp.dot(
                kv[slot, zc, 1], weights.astype(jnp.bfloat16), preferred_element_type=jnp.float32
            )

    def chunk(slot, zc):
        if slot == 0:
            block(zc, slot, zc, True)
            low = zc + 1
        else:
            theirs = 2 * lax.rem(y + slot // 2, 4) + (c if slot % 2 == 0 else other)
            low = zc + jnp.where(theirs > own, 1, 0)

        def step(zq, carry):
            block(zq, slot, zc, False)
            return carry

        lax.fori_loop(low, 4, step, 0)

    at = [lax.rem(z + d, 4) for d in ORDER]
    for t in range(4):
        arrived(kv.at[0, at[t]], zs_recv.at[at[t]])
        to_neighbour(0, at[t], 6, right, t).start()
        to_neighbour(0, at[t], 2, left, 4 + t).start()
        to_partner(0, at[t]).start()
    for t in range(4):
        arrived(q.at[at[t]], zq_recv.at[at[t]])

    def over(slot, t):
        chunk(slot, at[t])

    for t in range(4):
        over(0, t)
    for t in range(4):
        wait_chunk(1, at[t])
        over(1, t)
    for t in range(4):
        wait_chunk(6, at[t])
        if t < 2:
            to_neighbour(6, at[t], 4, right, 8 + t).start()
        to_partner(6, at[t]).start()
        wait_chunk(2, at[t])
        if t >= 2:
            to_neighbour(2, at[t], 4, left, 8 + t).start()
        to_partner(2, at[t]).start()
        over(6, t)
        over(2, t)
        if t:
            wait_chunk(7, at[t - 1])
            over(7, t - 1)
            wait_chunk(3, at[t - 1])
            over(3, t - 1)
    wait_chunk(7, at[3])
    over(7, 3)
    wait_chunk(3, at[3])
    over(3, 3)
    for t in (0, 2, 1, 3):
        wait_chunk(4, at[t])
        to_partner(4, at[t]).start()
        over(4, t)
    for t in (0, 2, 1, 3):
        wait_chunk(5, at[t])
        over(5, t)

    for dz in ORDER:
        zz = lax.rem(z + dz, 4)
        differ = acc[zz, 0] / total[zz, 0, 0:1] - lam_ref[0:1] * (acc[zz, 1] / total[zz, 1, 0:1])
        scale = lax.rsqrt(jnp.mean(differ * differ, axis=0, keepdims=True) + EPS)
        done_out[zz] = (differ * scale * gain_ref[...]).astype(jnp.bfloat16)
        if dz == 0:
            pltpu.make_async_copy(done_out.at[zz], back.at[z], back_recv.at[z]).start()
        else:
            pltpu.make_async_remote_copy(
                src_ref=done_out.at[zz],
                dst_ref=back.at[z],
                send_sem=back_send.at[dz],
                recv_sem=back_recv.at[z],
                device_id={"sp_0": zz},
                device_id_type=MESH,
            ).start()
    for dz in (0, 1, 3, 2):
        zz = lax.rem(z + dz, 4)
        arrived(back.at[zz], back_recv.at[zz])
        out_ref[zz] = back[zz]

    for j in range(4):
        mine = jnp.logical_and(2 * c + j // 2 == z, c == j % 2)

        @pl.when(jnp.logical_not(mine))
        def _():
            arrived(kv_in.at[j], zs_send.at[j])
            arrived(q_in.at[j], zq_send.at[j])

    for k in range(12):
        arrived(kv.at[0, 0], ring_send.at[k])
    for s in range(4):
        for t in range(4):
            arrived(kv.at[0, 0], core_send.at[s, t])
    for dz in range(1, 4):
        arrived(done_out.at[0], back_send.at[dz])


def attention(kv_in, q_in, lam_tile, gain_col):
    vmem = pl.BlockSpec(memory_space=pltpu.VMEM)
    dma = pltpu.SemaphoreType.DMA
    return pl.pallas_call(
        attention_kernel,
        out_shape=jax.ShapeDtypeStruct((4, PAIR, HALF), jnp.bfloat16),
        in_specs=[vmem] * 4,
        out_specs=vmem,
        scratch_shapes=[
            pltpu.VMEM((8, 4, 2, HALF, PAIR), jnp.bfloat16),
            pltpu.VMEM((4, PAIR, HALF), jnp.bfloat16),
            pltpu.VMEM((4, 2, PAIR, HALF), jnp.float32),
            pltpu.VMEM((4, 2, 8, HALF), jnp.float32),
            pltpu.VMEM((4, 2, 8, HALF), jnp.float32),
            pltpu.VMEM((4, PAIR, HALF), jnp.bfloat16),
            pltpu.VMEM((4, PAIR, HALF), jnp.bfloat16),
            dma((4,)),
            dma((4,)),
            dma((4,)),
            dma((4,)),
            dma((12,)),
            dma((8, 4)),
            dma((4, 4)),
            dma((4,)),
            dma((4,)),
        ],
        compiler_params=pltpu.CompilerParams(
            collective_id=0, has_side_effects=True, vmem_limit_bytes=40 * 2**20
        ),
    )(kv_in, q_in, lam_tile, gain_col)


def gathered_total(x, axis):
    return lax.all_gather(x, axis).sum(0)


def laid_out(parts, dim):
    lengths = list(parts.shape[1:])
    lengths[dim] *= parts.shape[0]
    return jnp.moveaxis(parts, 0, dim).reshape(lengths)


def copy_for_each(x, axis):
    length = lax.axis_size(axis)
    return lax.all_to_all(jnp.broadcast_to(x[None], (length, *x.shape)), axis, 0, 0, tiled=True)


def collect(x, axis, dim):
    return laid_out(copy_for_each(x, axis), dim)


def from_behind(x, axis, by):
    length = lax.axis_size(axis)
    pairs = [(i, i + by) for i in range(length) if 0 <= i + by < length]
    return lax.ppermute(x, axis, pairs)


def nothing_yet(x, identity):
    return jax.tree.map(
        lambda a, e: jnp.broadcast_to(jnp.asarray(e, a.dtype), a.shape), x, identity
    )


def prefix_by_axis(x, axes, combine, identity):
    before = start = nothing_yet(x, identity)
    running = x
    for axis in reversed(axes):
        length, index = (lax.axis_size(axis), lax.axis_index(axis))
        pieces = jax.tree.map(
            lambda part, kind: lax.all_gather(part.astype(kind), axis),
            running,
            (jnp.bfloat16, jnp.bfloat16),
        )
        inside, running = (start, start)
        for k in range(length):
            passed = k < index
            running = combine(
                running, jax.tree.map(lambda part, own: part[k].astype(own.dtype), pieces, x)
            )
            inside = jax.tree.map(lambda new, old: jnp.where(passed, new, old), running, inside)
        before = combine(inside, before)
    return before


def side_by_side(arrays, axis, dim, along):
    both = jnp.concatenate(arrays, axis=along)
    filled, at, gathered = (lax.all_gather(both, axis, axis=dim, tiled=True), 0, [])
    for a in arrays:
        gathered.append(lax.slice_in_dim(filled, at, at + a.shape[along], axis=along))
        at += a.shape[along]
    return tuple(gathered)


def per_device(
    hidden_in,
    in_gain,
    w_query,
    w_key,
    w_value,
    w_gate,
    w_inner,
    w_bvec,
    w_cvec,
    w_step,
    conv_inner,
    conv_bvec,
    conv_cvec,
    a_log,
    decay_add,
    lambdas,
    head_gain,
    ssm_gain,
    out_attn,
    out_ssm,
):
    rows_dev, half_width = hidden_in.shape
    in_float = hidden_in.astype(jnp.float32)
    squares = gathered_total(jnp.sum(in_float * in_float, axis=1), "tp")
    gain_half = lax.dynamic_slice_in_dim(in_gain, lax.axis_index("tp") * half_width, half_width, 0)
    normed = (in_float * lax.rsqrt(squares[:, None] / D + EPS) * gain_half[None, :]).astype(
        jnp.bfloat16
    )
    whole = collect(normed, "tp", 1)
    weight_list = (w_query, w_key, w_value, w_gate, w_inner, w_bvec, w_cvec, w_step)
    query, keys, values, gate_z, inner, b_pre, c_pre, step_pre = [
        jnp.dot(whole, weight, preferred_element_type=jnp.float32).astype(jnp.bfloat16)
        for weight in weight_list
    ]
    kv_in = jnp.stack(
        [
            jnp.stack(
                [
                    keys[r * HALF : (r + 1) * HALF, i * PAIR : (i + 1) * PAIR],
                    values[r * HALF : (r + 1) * HALF, i * PAIR : (i + 1) * PAIR].T,
                ]
            )
            for i in range(2)
            for r in range(2)
        ]
    )
    q_in = jnp.stack(
        [
            query[r * HALF : (r + 1) * HALF, i * PAIR : (i + 1) * PAIR].T
            for i in range(2)
            for r in range(2)
        ]
    )
    lam_all = lax.all_gather(lambdas, "tp", tiled=True)
    lam_tile = jnp.broadcast_to(
        lax.dynamic_slice_in_dim(lam_all, lax.axis_index("sp_0"), 1, 0)[:, None], (8, 256)
    )
    attn_cols = attention(kv_in, q_in, lam_tile, head_gain.reshape(PAIR, 1))
    heads_ssm = a_log.shape[0]
    groups_local = b_pre.shape[1] // STATE
    per_group = heads_ssm // groups_local
    stacked = jnp.concatenate([inner, b_pre, c_pre], axis=1)
    taps = conv_inner.shape[0]
    earlier = from_behind(stacked[rows_dev - (taps - 1) :], SP, 1)
    padded = jnp.concatenate([earlier, stacked], axis=0).astype(jnp.float32)
    conv_weight = jnp.concatenate([conv_inner, conv_bvec, conv_cvec], axis=1).astype(jnp.float32)
    summed = padded[0:rows_dev] * conv_weight[0]
    for offset in range(1, taps):
        summed = summed + padded[offset : offset + rows_dev] * conv_weight[offset]
    activated = jax.nn.silu(summed).astype(jnp.bfloat16)
    width_inner = inner.shape[1]
    width_vec = b_pre.shape[1]
    block_count = rows_dev // BLOCK
    inputs_x = activated[:, :width_inner].reshape(block_count, BLOCK, heads_ssm, SSM_P)
    inputs_b = activated[:, width_inner : width_inner + width_vec].reshape(
        block_count, BLOCK, groups_local, STATE
    )
    inputs_c = activated[:, width_inner + width_vec :].reshape(
        block_count, BLOCK, groups_local, STATE
    )
    step_size = jax.nn.softplus(step_pre.astype(jnp.float32))
    log_decay = -jnp.exp(a_log)[None, :] * step_size + decay_add
    size_major = step_size.reshape(block_count, BLOCK, heads_ssm).transpose(0, 2, 1)
    running = jnp.cumsum(
        log_decay.reshape(block_count, BLOCK, heads_ssm).transpose(0, 2, 1), axis=2
    )
    causal = jnp.tril(jnp.ones((BLOCK, BLOCK), dtype=bool))
    decay = jnp.exp(
        jnp.where(causal[None, None], running[:, :, :, None] - running[:, :, None, :], NEG)
    )
    intersection = jnp.einsum(
        "ntgk,nsgk->ngts", inputs_c, inputs_b, preferred_element_type=jnp.float32
    )
    matrix = (
        jnp.repeat(intersection, per_group, axis=1) * decay * size_major[:, :, None, :]
    ).astype(jnp.bfloat16)
    inside = jnp.einsum("nhts,nshp->nthp", matrix, inputs_x, preferred_element_type=jnp.float32)
    to_end = (jnp.exp(running[:, :, -1:] - running) * size_major).transpose(0, 2, 1)
    weighted = (inputs_x.astype(jnp.float32) * to_end[..., None]).astype(jnp.bfloat16)
    heads_b = jnp.repeat(inputs_b, per_group, axis=2)
    fresh = jnp.einsum("nshp,nshk->nhpk", weighted, heads_b, preferred_element_type=jnp.float32)
    block_totals = running[:, :, -1]

    def chain(state, items):
        fresh_block, total_block = items
        return (state * jnp.exp(total_block)[:, None, None] + fresh_block, state)

    local_end, local_enter = lax.scan(
        chain, jnp.zeros((heads_ssm, SSM_P, STATE), jnp.float32), (fresh, block_totals)
    )
    device_total = jnp.sum(block_totals, axis=0)

    def link(before, after):
        return (before[0] * jnp.exp(after[1])[:, None, None] + after[0], before[1] + after[1])

    incoming, skipped = prefix_by_axis(
        (local_end, device_total),
        SP,
        link,
        (jnp.zeros_like(local_end), jnp.zeros_like(device_total)),
    )
    preceding = jnp.concatenate(
        [jnp.zeros((1, heads_ssm), jnp.float32), jnp.cumsum(block_totals, axis=0)[:-1]], axis=0
    )
    entering = local_enter + incoming[None] * jnp.exp(preceding)[:, :, None, None]
    heads_c = jnp.repeat(inputs_c, per_group, axis=2).astype(jnp.float32)
    carried = (
        jnp.einsum("nthk,nhpk->nthp", heads_c, entering, precision=lax.Precision.HIGHEST)
        * jnp.exp(running).transpose(0, 2, 1)[..., None]
    )
    ssm_y = (inside + carried).reshape(rows_dev, heads_ssm * SSM_P)
    gated = (ssm_y * jax.nn.silu(gate_z.astype(jnp.float32))).reshape(rows_dev, groups_local, -1)
    grouped = gated * lax.rsqrt(jnp.mean(gated * gated, axis=-1, keepdims=True) + EPS)
    ssm_out = (grouped.reshape(rows_dev, heads_ssm * SSM_P) * ssm_gain).astype(jnp.bfloat16)
    ssm_rows = lax.all_to_all(ssm_out, "tp", split_axis=0, concat_axis=1, tiled=True)
    full_attn, full_ssm = side_by_side((out_attn, out_ssm), "tp", 0, 1)
    joined = jnp.einsum(
        "hcq,hcd->qd", attn_cols, full_attn.reshape(4, PAIR, D), preferred_element_type=jnp.float32
    ) + jnp.dot(ssm_rows, full_ssm, preferred_element_type=jnp.float32)
    return joined.astype(jnp.bfloat16)


def solution(mesh):
    split = Mesh(
        mesh.devices.reshape(4, 4, mesh.shape["fs"], mesh.shape["tp"]), ("sp_0", "sp_1", "fs", "tp")
    )
    in_specs = (
        P(FS_SP, "tp"),
        P(),
        P(None, "tp"),
        P(None, "tp"),
        P(None, "tp"),
        P(None, "tp"),
        P(None, "tp"),
        P(None, "tp"),
        P(None, "tp"),
        P(None, "tp"),
        P(None, "tp"),
        P(None, "tp"),
        P(None, "tp"),
        P("tp"),
        P(FS_SP, "tp"),
        P("tp"),
        P(),
        P("tp"),
        P("tp", None),
        P("tp", None),
    )
    out_specs = P(FS_SP_TP, None)
    return jax.shard_map(
        per_device, mesh=split, in_specs=in_specs, out_specs=out_specs, check_vma=False
    )
```

```python
import jax
import jax.numpy as jnp
from jax import lax
from jax.experimental import pallas as pl
from jax.experimental.pallas import tpu as pltpu
from jax.sharding import Mesh
from jax.sharding import PartitionSpec as P

D = 2048
QK_DIM = 128
SSM_P = 64
STATE = 128
BLOCK = 128
ROWS = 512
HALF = 256
PAIR = 256
FS_SP = ("fs", "sp_0", "sp_1")
FS_SP_TP = ("fs", "sp_0", "sp_1", "tp")
MESH = pl.DeviceIdType.MESH
ORDER = (0, 1, 3, 2)
SCALE2 = QK_DIM ** (-0.5) * 1.4426950408889634
EPS = 1e-06
NEG = -1e30
F32, BF16 = jnp.float32, jnp.bfloat16


def matmul(a, b):
    return jnp.dot(a, b, preferred_element_type=F32)


def contract(a, b, da, db):
    return lax.dot_general(a, b, (((da,), (db,)), ((), ())), preferred_element_type=F32)


def arrived(ref, sem):
    pltpu.make_async_copy(ref, ref, sem).wait()


def layer_kernel(
    hidden,
    in_gain,
    w_query,
    w_key,
    w_value,
    w_gate,
    w_inner,
    w_bvec,
    w_cvec,
    w_step,
    conv_inner,
    conv_bvec,
    conv_cvec,
    a_log,
    decay_add,
    lambdas,
    head_gain,
    ssm_gain,
    out_attn,
    out_ssm,
    out_ref,
    x,
    normed,
    wq,
    wk,
    wv,
    wg,
    wx,
    wb,
    wc,
    ws,
    wo,
    kv_in,
    q_in,
    kv,
    q,
    acc,
    peak,
    total,
    done_out,
    back,
    pre,
    halo_out,
    halo_in,
    act,
    gate,
    narrow,
    cols,
    ysum,
    state,
    st_out,
    tot_out,
    st_y,
    tot_y,
    row_out,
    rtot_out,
    st_z,
    tot_z,
    ssm_all,
    ssm_buf,
    joined,
    lam_own,
    lam_in,
    load_sem,
    x_sem,
    wo_sem,
    zs_send,
    zs_recv,
    zq_send,
    zq_recv,
    ring_send,
    kv_recv,
    core_send,
    back_send,
    back_recv,
    halo_sem,
    sty_send,
    sty_recv,
    stz_send,
    stz_recv,
    ssm_sem,
    lam_sem,
):
    z, y, c = lax.axis_index("sp_0"), lax.axis_index("sp_1"), lax.axis_index("tp")
    right, left = lax.rem(y + 1, 4), lax.rem(y + 3, 4)
    other = 1 - c
    next_z = lax.rem(z + jnp.where(y == 3, 1, 0), 4)
    prev_z = lax.rem(z + jnp.where(y == 0, 3, 0), 4)

    loads = []
    for k, (src, dst) in enumerate(
        (
            (hidden, x.at[c]),
            (w_key, wk),
            (w_value, wv),
            (w_query, wq),
            (w_inner, wx),
            (w_bvec, wb),
            (w_cvec, wc),
            (w_gate, wg),
            (w_step, ws),
            (out_ssm, wo.at[c, 1]),
            (out_attn, wo.at[c, 0]),
        )
    ):
        loads.append(pltpu.make_async_copy(src, dst, load_sem.at[k]))
        loads[-1].start()

    barrier = pltpu.get_barrier_semaphore()

    def greet(where):
        pl.semaphore_signal(barrier, inc=1, device_id=where, device_id_type=MESH)

    for dz in range(4):
        for dc in range(2):
            if dz or dc:
                greet({"sp_0": lax.rem(z + dz, 4), "tp": lax.rem(c + dc, 2)})
    for dy in range(1, 4):
        greet({"sp_1": lax.rem(y + dy, 4)})
    greet({"sp_0": next_z, "sp_1": right})
    greet({"sp_0": prev_z, "sp_1": left})
    pl.semaphore_wait(barrier, 12)

    def remote(src, dst, send, recv, where):
        return pltpu.make_async_remote_copy(
            src_ref=src,
            dst_ref=dst,
            send_sem=send,
            recv_sem=recv,
            device_id=where,
            device_id_type=MESH,
        )

    x_copy = remote(hidden, x.at[c], x_sem.at[0], x_sem.at[1], {"tp": other})
    x_copy.start()

    acc[...] = jnp.zeros_like(acc)
    total[...] = jnp.zeros_like(total)
    peak[...] = jnp.full_like(peak, NEG)
    narrow[...] = jnp.zeros_like(narrow)
    for i in range(2):
        lam_own[i] = jnp.full((8, 128), lambdas[0, i], F32)
    lam_copy = remote(lam_own, lam_in, lam_sem.at[0], lam_sem.at[1], {"tp": other})
    lam_copy.start()

    loads[0].wait()
    arrived(x.at[other], x_sem.at[1])

    def norm_rows(n, carry):
        rows = pl.ds(pl.multiple_of(n * 64, 64), 64)
        first, second = x[0, rows, :].astype(F32), x[1, rows, :].astype(F32)
        squares = jnp.sum(first * first, axis=1, keepdims=True) + jnp.sum(
            second * second, axis=1, keepdims=True
        )
        scale = lax.rsqrt(squares / D + EPS)
        normed[rows, 0:1024] = (first * scale * in_gain[:, 0:1024]).astype(BF16)
        normed[rows, 1024:2048] = (second * scale * in_gain[:, 1024:2048]).astype(BF16)
        return carry

    lax.fori_loop(0, 8, norm_rows, 0)

    wo_copies = [
        remote(out_ssm, wo.at[c, 1], wo_sem.at[0], wo_sem.at[1], {"tp": other}),
        remote(out_attn, wo.at[c, 0], wo_sem.at[2], wo_sem.at[3], {"tp": other}),
    ]

    def exchange(src, dst, send, recv, j):
        to, r = 2 * c + j // 2, j % 2
        mine = jnp.logical_and(to == z, c == r)

        @pl.when(mine)
        def _():
            pltpu.make_async_copy(src.at[j], dst, recv.at[z]).start()

        @pl.when(jnp.logical_not(mine))
        def _():
            remote(src.at[j], dst, send.at[j], recv.at[z], {"sp_0": to, "tp": r}).start()

    loads[1].wait()
    loads[2].wait()
    for i in range(2):
        lanes = slice(i * PAIR, (i + 1) * PAIR)
        keys = matmul(normed[...], wk[:, lanes])
        for r in range(2):
            kv_in[2 * i + r, 0] = keys[r * HALF : (r + 1) * HALF].astype(BF16)
        values = matmul(normed[...], wv[:, lanes])
        for r in range(2):
            kv_in[2 * i + r, 1] = values[r * HALF : (r + 1) * HALF].T.astype(BF16)
        for r in range(2):
            exchange(kv_in, kv.at[0, z], zs_send, zs_recv, 2 * i + r)
    for copy in wo_copies:
        copy.start()
    loads[3].wait()
    for i in range(2):
        queries = matmul(normed[...], wq[:, i * PAIR : (i + 1) * PAIR])
        for r in range(2):
            q_in[2 * i + r] = queries[r * HALF : (r + 1) * HALF].T.astype(BF16)
            exchange(q_in, q.at[z], zq_send, zq_recv, 2 * i + r)

    def to_neighbour(slot, zz, new_slot, yy, k):
        return remote(
            kv.at[slot, zz],
            kv.at[new_slot, zz],
            ring_send.at[k],
            kv_recv.at[new_slot, zz],
            {"sp_1": yy},
        )

    def to_partner(slot, zz):
        return remote(
            kv.at[slot, zz],
            kv.at[slot + 1, zz],
            core_send.at[slot // 2, zz],
            kv_recv.at[slot + 1, zz],
            {"tp": other},
        )

    at = [lax.rem(z + d, 4) for d in ORDER]

    def serve(t):
        arrived(kv.at[0, at[t]], zs_recv.at[at[t]])
        to_neighbour(0, at[t], 6, right, t).start()
        to_neighbour(0, at[t], 2, left, 4 + t).start()
        to_partner(0, at[t]).start()

    serve(0)

    for k in (4, 5, 6):
        loads[k].wait()
    for wide, lanes, at_lane in (
        (wx, slice(0, 256), 0),
        (wx, slice(256, 512), 256),
        (wb, slice(0, 256), 512),
        (wc, slice(0, 256), 768),
    ):
        part = matmul(normed[...], wide[:, lanes]).astype(BF16)
        pre[8:520, at_lane : at_lane + 256] = part.astype(F32)
        halo_out[:, at_lane : at_lane + 256] = part[496:512]
    halo_copy = remote(
        halo_out, halo_in, halo_sem.at[0], halo_sem.at[1], {"sp_0": next_z, "sp_1": right}
    )
    halo_copy.start()
    loads[7].wait()
    for i in range(2):
        lanes = slice(i * 256, (i + 1) * 256)
        gate[:, lanes] = matmul(normed[...], wg[:, lanes]).astype(BF16)
    loads[8].wait()
    narrow[0, :, 0:8] = matmul(normed[...], ws[...]).astype(BF16).astype(F32)
    narrow[1, :, 0:8] = decay_add[...]
    arrived(halo_in, halo_sem.at[1])
    begins = jnp.logical_and(z == 0, y == 0)
    pre[0:8, :] = halo_in[...].astype(F32)[8:16] * jnp.where(begins, 0.0, 1.0)
    for at_lane, (taps, lanes) in enumerate(
        (
            (conv_inner, slice(0, 256)),
            (conv_inner, slice(256, 512)),
            (conv_bvec, slice(0, 256)),
            (conv_cvec, slice(0, 256)),
        )
    ):
        here = slice(at_lane * 256, at_lane * 256 + 256)
        weight = taps[:, lanes].astype(F32)
        for n in range(4):
            summed = pre[5 + n * BLOCK : 5 + (n + 1) * BLOCK, here] * weight[0:1]
            for o in range(1, 4):
                summed = (
                    summed + pre[5 + o + n * BLOCK : 5 + o + (n + 1) * BLOCK, here] * weight[o : o + 1]
                )
            act[n * BLOCK : (n + 1) * BLOCK, here] = (summed * jax.nn.sigmoid(summed)).astype(BF16)

    serve(1)

    rate = jnp.zeros((8, 128), F32)
    sub = lax.broadcasted_iota(jnp.int32, (8, 128), 0)
    lane8 = lax.broadcasted_iota(jnp.int32, (8, 128), 1)
    for h in range(8):
        rate = jnp.where(sub == h, a_log[0, h], rate)
    rate = -jnp.exp(rate)
    t_at = lax.broadcasted_iota(jnp.int32, (BLOCK, BLOCK), 0)
    s_at = lax.broadcasted_iota(jnp.int32, (BLOCK, BLOCK), 1)
    causal = s_at <= t_at
    low_lane = s_at < SSM_P
    quarter = lax.broadcasted_iota(jnp.int32, (BLOCK, 256), 1) // SSM_P

    def spread(tile, first):
        pairs = [
            jnp.where(low_lane, tile[:, first + a : first + a + 1], tile[:, first + a + 1 : first + a + 2])
            for a in (0, 2)
        ]
        return jnp.concatenate(pairs, axis=1)

    def by_head(tile):
        return jnp.concatenate(
            [jnp.broadcast_to(tile[h : h + 1], (SSM_P, 128)) for h in range(tile.shape[0])], axis=0
        )

    def split_dot(left_side, right_side):
        high = right_side.astype(BF16)
        low = (right_side - high.astype(F32)).astype(BF16)
        return contract(left_side, high, 1, 1) + contract(left_side, low, 1, 1)

    state[...] = jnp.zeros_like(state)
    preceding = jnp.zeros((8, 128), F32)
    for n in range(4):
        rows = slice(n * BLOCK, (n + 1) * BLOCK)
        step_pre = narrow[0, rows, :].T[0:8]
        decay_row = narrow[1, rows, :].T[0:8]
        size = jnp.maximum(step_pre, 0.0) + jnp.log1p(jnp.exp(-jnp.abs(step_pre)))
        running = rate * size + decay_row
        for shift in (1, 2, 4, 8, 16, 32, 64):
            running = running + jnp.where(lane8 >= shift, pltpu.roll(running, shift, 1), 0.0)
        last = jnp.broadcast_to(running[:, 127:128], (8, 128))
        to_end = jnp.exp(last - running) * size
        tall = jnp.concatenate(
            [running, to_end, jnp.exp(running), jnp.exp(running + preceding), jnp.zeros((96, 128), F32)],
            axis=0,
        ).T
        cols[rows, :] = tall
        keep = jnp.exp(last)
        preceding = preceding + last
        for g in range(2):
            lanes = slice(g * 256, (g + 1) * 256)
            inputs_x = act[rows, lanes]
            inputs_b = act[rows, 512 + g * 128 : 640 + g * 128]
            inputs_c = act[rows, 768 + g * 128 : 896 + g * 128]
            crossing = contract(inputs_c, inputs_b, 1, 1)
            mixes, own_x = [], []
            for a in range(4):
                h = 4 * g + a
                fade = jnp.exp(
                    jnp.where(causal, tall[:, h : h + 1] - running[h : h + 1, :], NEG)
                )
                mixes.append((crossing * fade * size[h : h + 1, :]).astype(BF16))
                own_x.append(jnp.where(quarter == a, inputs_x, jnp.zeros_like(inputs_x)))
            inside = matmul(jnp.concatenate(mixes, axis=1), jnp.concatenate(own_x, axis=0))
            weighted = (inputs_x.astype(F32) * spread(tall, 8 + 4 * g)).astype(BF16)
            fresh = contract(weighted, inputs_b, 0, 0)
            before = state[lanes, :]
            carried = split_dot(inputs_c, before) * spread(tall, 16 + 4 * g)
            ysum[rows, lanes] = inside + carried
            state[lanes, :] = before * by_head(keep[4 * g : 4 * g + 4]) + fresh
    st_out[...] = state[...].astype(BF16)
    tot_out[...] = preceding
    st_y[y] = state[...].astype(BF16)
    tot_y[y] = preceding
    for dy in range(1, 4):
        where = {"sp_1": lax.rem(y + dy, 4)}
        remote(st_out, st_y.at[y], sty_send.at[0, dy], sty_recv.at[0, y], where).start()
        remote(tot_out, tot_y.at[y], sty_send.at[1, dy], sty_recv.at[1, y], where).start()

    serve(2)
    serve(3)

    def wait_chunk(slot, zz):
        arrived(kv.at[slot, zz], kv_recv.at[slot, zz])

    own = 2 * y + c

    def block(zq, slot, zc, masked):
        for m in range(2):
            lanes = slice(m * QK_DIM, (m + 1) * QK_DIM)
            scores = matmul(kv[slot, zc, 0, :, lanes], q[zq, lanes, :]) * SCALE2
            if masked:
                key_at = lax.broadcasted_iota(jnp.int32, scores.shape, 0)
                query_at = lax.broadcasted_iota(jnp.int32, scores.shape, 1)
                scores = jnp.where(key_at <= query_at, scores, NEG)
            old = peak[zq, m]
            new = jnp.maximum(old, jnp.max(scores, axis=0, keepdims=True))
            weights = jnp.exp2(scores - new[0:1])
            shrink = jnp.exp2(old - new)
            peak[zq, m] = new
            total[zq, m] = total[zq, m] * shrink + jnp.sum(weights, axis=0, keepdims=True)
            acc[zq, m] = acc[zq, m] * shrink[0:1] + matmul(kv[slot, zc, 1], weights.astype(BF16))

    def over(slot, t):
        zc = at[t]
        if slot == 0:
            block(zc, slot, zc, True)
            low = zc + 1
        else:
            theirs = 2 * lax.rem(y + slot // 2, 4) + (c if slot % 2 == 0 else other)
            low = zc + jnp.where(theirs > own, 1, 0)

        def step(zq, carry):
            block(zq, slot, zc, False)
            return carry

        lax.fori_loop(low, 4, step, 0)

    def prefix(states, totals, mine, send_states, send_totals):
        run_s, run_t = jnp.zeros((512, 128), F32), jnp.zeros((8, 128), F32)
        before_s, before_t = run_s, run_t
        for k in range(4):
            run_s = run_s * by_head(jnp.exp(totals[k])) + states[k].astype(F32)
            run_t = run_t + totals[k]
            before_s = jnp.where(k < mine, run_s, before_s)
            before_t = jnp.where(k < mine, run_t, before_t)
        if send_states is not None:
            send_states[...] = run_s.astype(BF16)
            send_totals[...] = run_t
            st_z[z] = run_s.astype(BF16)
            tot_z[z] = run_t
        return before_s, before_t

    for t in range(4):
        arrived(q.at[at[t]], zq_recv.at[at[t]])
    for t in range(4):
        over(0, t)
    for dy in range(1, 4):
        yy = lax.rem(y + dy, 4)
        arrived(st_y.at[yy], sty_recv.at[0, yy])
        arrived(tot_y.at[yy], sty_recv.at[1, yy])
    row_before, row_total = prefix(st_y, tot_y, y, row_out, rtot_out)
    state[...] = row_before
    tot_out2 = row_total
    for dz in range(1, 4):
        where = {"sp_0": lax.rem(z + dz, 4)}
        remote(row_out, st_z.at[z], stz_send.at[0, dz], stz_recv.at[0, z], where).start()
        remote(rtot_out, tot_z.at[z], stz_send.at[1, dz], stz_recv.at[1, z], where).start()
    for t in range(4):
        wait_chunk(1, at[t])
        over(1, t)

    def finish_ssm():
        for dz in range(1, 4):
            zz = lax.rem(z + dz, 4)
            arrived(st_z.at[zz], stz_recv.at[0, zz])
            arrived(tot_z.at[zz], stz_recv.at[1, zz])
        far, _ = prefix(st_z, tot_z, z, None, None)
        state[...] = far * by_head(jnp.exp(tot_out2)) + state[...]
        for n in range(4):
            rows = slice(n * BLOCK, (n + 1) * BLOCK)
            for g in range(2):
                lanes = slice(g * 256, (g + 1) * 256)
                inputs_c = act[rows, 768 + g * 128 : 896 + g * 128]
                value = ysum[rows, lanes] + split_dot(inputs_c, state[lanes, :]) * spread(
                    cols[rows, :], 24 + 4 * g
                )
                opened = gate[rows, lanes].astype(F32)
                value = value * (opened * jax.nn.sigmoid(opened))
                scale = lax.rsqrt(jnp.mean(value * value, axis=1, keepdims=True) + EPS)
                ssm_all[n // 2, (n % 2) * BLOCK : (n % 2 + 1) * BLOCK, lanes] = (
                    value * scale * ssm_gain[:, lanes]
                ).astype(BF16)
        ssm_buf[c] = ssm_all[c]
        remote(ssm_all.at[other], ssm_buf.at[c], ssm_sem.at[0], ssm_sem.at[1], {"tp": other}).start()

    def project_ssm():
        arrived(ssm_buf.at[other], ssm_sem.at[1])
        loads[9].wait()
        arrived(wo.at[other, 1], wo_sem.at[1])
        for k in range(4):
            lanes = slice(k * 512, (k + 1) * 512)
            joined[:, lanes] = matmul(ssm_buf[0], wo[0, 1, :, lanes]) + matmul(
                ssm_buf[1], wo[1, 1, :, lanes]
            )

    for t in range(4):
        wait_chunk(6, at[t])
        if t < 2:
            to_neighbour(6, at[t], 4, right, 8 + t).start()
        to_partner(6, at[t]).start()
        wait_chunk(2, at[t])
        if t >= 2:
            to_neighbour(2, at[t], 4, left, 8 + t).start()
        to_partner(2, at[t]).start()
        over(6, t)
        over(2, t)
        if t:
            wait_chunk(7, at[t - 1])
            over(7, t - 1)
            wait_chunk(3, at[t - 1])
            over(3, t - 1)
        if t == 0:
            finish_ssm()
        if t == 1:
            project_ssm()
    wait_chunk(7, at[3])
    over(7, 3)
    wait_chunk(3, at[3])
    over(3, 3)
    for t in (0, 2, 1, 3):
        wait_chunk(4, at[t])
        to_partner(4, at[t]).start()
        over(4, t)
    for t in (0, 2, 1, 3):
        wait_chunk(5, at[t])
        over(5, t)

    arrived(lam_in, lam_sem.at[1])
    held = jnp.where(z // 2 == c, lam_own[lax.rem(z, 2)], lam_in[lax.rem(z, 2)])
    lam = jnp.concatenate([held, held], axis=1)[0:1]
    gain_col = jnp.broadcast_to(head_gain[...], (PAIR, PAIR)).T
    for dz in ORDER:
        zz = lax.rem(z + dz, 4)
        differ = acc[zz, 0] / total[zz, 0, 0:1] - lam * (acc[zz, 1] / total[zz, 1, 0:1])
        scale = lax.rsqrt(jnp.mean(differ * differ, axis=0, keepdims=True) + EPS)
        done_out[zz] = (differ * scale * gain_col).astype(BF16)
        if dz == 0:
            back[zz] = done_out[zz]
        else:
            remote(
                done_out.at[zz], back.at[z], back_send.at[dz], back_recv.at[z], {"sp_0": zz}
            ).start()
    loads[10].wait()
    arrived(wo.at[other, 0], wo_sem.at[3])
    for dz in range(1, 4):
        zz = lax.rem(z + dz, 4)
        arrived(back.at[zz], back_recv.at[zz])
    for k in range(4):
        lanes = slice(k * 512, (k + 1) * 512)
        sum_k = joined[:, lanes]
        for h in range(4):
            sum_k = sum_k + contract(
                back[h], wo[h // 2, 0, (h % 2) * PAIR : (h % 2 + 1) * PAIR, lanes], 0, 0
            )
        out_ref[:, lanes] = sum_k.astype(BF16)

    x_copy.wait_send()
    lam_copy.wait_send()
    halo_copy.wait_send()
    for copy in wo_copies:
        copy.wait_send()
    for j in range(4):
        mine = jnp.logical_and(2 * c + j // 2 == z, c == j % 2)

        @pl.when(jnp.logical_not(mine))
        def _():
            arrived(kv_in.at[j], zs_send.at[j])
            arrived(q_in.at[j], zq_send.at[j])

    for k in range(12):
        arrived(kv.at[0, 0], ring_send.at[k])
    for s in range(4):
        for t in range(4):
            arrived(kv.at[0, 0], core_send.at[s, t])
    for d in range(1, 4):
        arrived(done_out.at[0], back_send.at[d])
        arrived(st_out, sty_send.at[0, d])
        arrived(tot_out, sty_send.at[1, d])
        arrived(row_out, stz_send.at[0, d])
        arrived(rtot_out, stz_send.at[1, d])
    arrived(ssm_all.at[0], ssm_sem.at[0])


def per_device(
    hidden_in,
    in_gain,
    w_query,
    w_key,
    w_value,
    w_gate,
    w_inner,
    w_bvec,
    w_cvec,
    w_step,
    conv_inner,
    conv_bvec,
    conv_cvec,
    a_log,
    decay_add,
    lambdas,
    head_gain,
    ssm_gain,
    out_attn,
    out_ssm,
):
    vmem = pl.BlockSpec(memory_space=pltpu.VMEM)
    smem = pl.BlockSpec(memory_space=pltpu.SMEM)
    away = pl.BlockSpec(memory_space=pl.ANY)
    dma = pltpu.SemaphoreType.DMA
    buf = pltpu.VMEM
    return pl.pallas_call(
        layer_kernel,
        out_shape=jax.ShapeDtypeStruct((HALF, D), BF16),
        in_specs=[away, vmem]
        + [away] * 8
        + [vmem] * 3
        + [smem, vmem, smem, vmem, vmem, away, away],
        out_specs=vmem,
        scratch_shapes=[
            buf((2, ROWS, 1024), BF16),
            buf((ROWS, D), BF16),
            buf((D, 512), BF16),
            buf((D, 512), BF16),
            buf((D, 512), BF16),
            buf((D, 512), BF16),
            buf((D, 512), BF16),
            buf((D, 256), BF16),
            buf((D, 256), BF16),
            buf((D, 8), BF16),
            buf((2, 2, 512, D), BF16),
            buf((4, 2, HALF, PAIR), BF16),
            buf((4, PAIR, HALF), BF16),
            buf((8, 4, 2, HALF, PAIR), BF16),
            buf((4, PAIR, HALF), BF16),
            buf((4, 2, PAIR, HALF), F32),
            buf((4, 2, 8, HALF), F32),
            buf((4, 2, 8, HALF), F32),
            buf((4, PAIR, HALF), BF16),
            buf((4, PAIR, HALF), BF16),
            buf((520, 1024), F32),
            buf((16, 1024), BF16),
            buf((16, 1024), BF16),
            buf((ROWS, 1024), BF16),
            buf((ROWS, 512), BF16),
            buf((2, ROWS, 128), F32),
            buf((ROWS, 128), F32),
            buf((ROWS, 512), F32),
            buf((512, 128), F32),
            buf((512, 128), BF16),
            buf((8, 128), F32),
            buf((4, 512, 128), BF16),
            buf((4, 8, 128), F32),
            buf((512, 128), BF16),
            buf((8, 128), F32),
            buf((4, 512, 128), BF16),
            buf((4, 8, 128), F32),
            buf((2, HALF, 512), BF16),
            buf((2, HALF, 512), BF16),
            buf((HALF, D), F32),
            buf((2, 8, 128), F32),
            buf((2, 8, 128), F32),
            dma((11,)),
            dma((2,)),
            dma((4,)),
            dma((4,)),
            dma((4,)),
            dma((4,)),
            dma((4,)),
            dma((12,)),
            dma((8, 4)),
            dma((4, 4)),
            dma((4,)),
            dma((4,)),
            dma((2,)),
            dma((2, 4)),
            dma((2, 4)),
            dma((2, 4)),
            dma((2, 4)),
            dma((2,)),
            dma((2,)),
        ],
        compiler_params=pltpu.CompilerParams(
            collective_id=0, has_side_effects=True, vmem_limit_bytes=63 * 2**20
        ),
    )(
        hidden_in,
        in_gain.reshape(1, D),
        w_query,
        w_key,
        w_value,
        w_gate,
        w_inner,
        w_bvec,
        w_cvec,
        w_step,
        conv_inner,
        conv_bvec,
        conv_cvec,
        a_log.reshape(1, 8),
        decay_add,
        lambdas.reshape(1, 2),
        head_gain.reshape(1, PAIR),
        ssm_gain.reshape(1, 512),
        out_attn,
        out_ssm,
    )


def solution(mesh):
    split = Mesh(
        mesh.devices.reshape(4, 4, mesh.shape["fs"], mesh.shape["tp"]), ("sp_0", "sp_1", "fs", "tp")
    )
    in_specs = (
        P(FS_SP, "tp"),
        P(),
        P(None, "tp"),
        P(None, "tp"),
        P(None, "tp"),
        P(None, "tp"),
        P(None, "tp"),
        P(None, "tp"),
        P(None, "tp"),
        P(None, "tp"),
        P(None, "tp"),
        P(None, "tp"),
        P(None, "tp"),
        P("tp"),
        P(FS_SP, "tp"),
        P("tp"),
        P(),
        P("tp"),
        P("tp", None),
        P("tp", None),
    )
    out_specs = P(FS_SP_TP, None)
    return jax.shard_map(
        per_device, mesh=split, in_specs=in_specs, out_specs=out_specs, check_vma=False
    )
```

```python
import jax
import jax.numpy as jnp
from jax import lax
from jax.experimental import pallas as pl
from jax.experimental.pallas import tpu as pltpu
from jax.sharding import Mesh
from jax.sharding import PartitionSpec as P

D = 2048
QK_DIM = 128
SSM_P = 64
STATE = 128
BLOCK = 128
ROWS = 512
HALF = 256
PAIR = 256
FS_SP = ("fs", "sp_0", "sp_1")
FS_SP_TP = ("fs", "sp_0", "sp_1", "tp")
MESH = pl.DeviceIdType.MESH
SCALE2 = QK_DIM ** (-0.5) * 1.4426950408889634
EPS = 1e-06
NEG = -1e30
F32, BF16 = jnp.float32, jnp.bfloat16


def matmul(a, b):
    return jnp.dot(a, b, preferred_element_type=F32)


def contract(a, b, da, db):
    return lax.dot_general(a, b, (((da,), (db,)), ((), ())), preferred_element_type=F32)


def arrived(ref, sem):
    pltpu.make_async_copy(ref, ref, sem).wait()


def layer_kernel(
    hidden,
    in_gain,
    w_query,
    w_key,
    w_value,
    w_gate,
    w_inner,
    w_bvec,
    w_cvec,
    w_step,
    conv_inner,
    conv_bvec,
    conv_cvec,
    a_log,
    decay_add,
    lambdas,
    head_gain,
    ssm_gain,
    out_attn,
    out_ssm,
    out_ref,
    x,
    normed,
    wq,
    wk,
    wv,
    wg,
    wx,
    wb,
    wc,
    ws,
    wo,
    kv_in,
    q_in,
    kv,
    q,
    acc,
    peak,
    total,
    done_out,
    back,
    pre,
    halo_out,
    halo_in,
    act,
    gate,
    narrow,
    cols,
    ysum,
    state,
    st_out,
    tot_out,
    st_y,
    tot_y,
    row_out,
    rtot_out,
    st_z,
    tot_z,
    pre_s,
    pre_t,
    inc_out,
    inc_in,
    ssm_all,
    ssm_buf,
    joined,
    lam_own,
    lam_in,
    gain_col,
    result,
    load_sem,
    x_sem,
    wo_sem,
    zs_send,
    zs_recv,
    zq_send,
    zq_recv,
    ring_send,
    kv_recv,
    core_send,
    back_send,
    back_recv,
    halo_sem,
    sty_send,
    sty_recv,
    stz_send,
    stz_recv,
    ssm_sem,
    lam_sem,
    out_sem,
    inc_send,
    inc_recv,
):
    z, y, c = lax.axis_index("sp_0"), lax.axis_index("sp_1"), lax.axis_index("tp")
    right, left = lax.rem(y + 1, 4), lax.rem(y + 3, 4)
    other = 1 - c
    next_z = lax.rem(z + jnp.where(y == 3, 1, 0), 4)
    prev_z = lax.rem(z + jnp.where(y == 0, 3, 0), 4)

    loads = []
    for k, (src, dst) in enumerate(
        (
            (hidden, x.at[c]),
            (w_key, wk),
            (w_value, wv),
            (w_query, wq),
            (w_inner, wx),
            (w_bvec, wb),
            (w_cvec, wc),
            (w_gate, wg),
            (w_step, ws),
            (out_ssm, wo.at[c, 1]),
            (out_attn, wo.at[c, 0]),
        )
    ):
        loads.append(pltpu.make_async_copy(src, dst, load_sem.at[k]))
        loads[-1].start()

    barrier = pltpu.get_barrier_semaphore()

    def greet(where):
        pl.semaphore_signal(barrier, inc=1, device_id=where, device_id_type=MESH)

    for dz in range(4):
        for dc in range(2):
            if dz or dc:
                greet({"sp_0": lax.rem(z + dz, 4), "tp": lax.rem(c + dc, 2)})
    for dy in range(1, 4):
        greet({"sp_1": lax.rem(y + dy, 4)})
    greet({"sp_0": next_z, "sp_1": right})
    greet({"sp_0": prev_z, "sp_1": left})
    pl.semaphore_wait(barrier, 12)

    def remote(src, dst, send, recv, where):
        return pltpu.make_async_remote_copy(
            src_ref=src,
            dst_ref=dst,
            send_sem=send,
            recv_sem=recv,
            device_id=where,
            device_id_type=MESH,
        )

    x_copy = remote(hidden, x.at[c], x_sem.at[0], x_sem.at[1], {"tp": other})
    x_copy.start()

    acc[...] = jnp.zeros_like(acc)
    total[...] = jnp.zeros_like(total)
    peak[...] = jnp.full_like(peak, NEG)
    for i in range(2):
        lam_own[i] = jnp.full((8, 128), lambdas[0, i], F32)
    lam_copy = remote(lam_own, lam_in, lam_sem.at[0], lam_sem.at[1], {"tp": other})
    lam_copy.start()

    loads[0].wait()
    arrived(x.at[other], x_sem.at[1])

    def norm_rows(n, carry):
        rows = pl.ds(pl.multiple_of(n * 64, 64), 64)
        first, second = x[0, rows, :].astype(F32), x[1, rows, :].astype(F32)
        squares = jnp.sum(first * first, axis=1, keepdims=True) + jnp.sum(
            second * second, axis=1, keepdims=True
        )
        scale = lax.rsqrt(squares / D + EPS)
        normed[rows, 0:1024] = (first * scale * in_gain[:, 0:1024]).astype(BF16)
        normed[rows, 1024:2048] = (second * scale * in_gain[:, 1024:2048]).astype(BF16)
        return carry

    lax.fori_loop(0, 8, norm_rows, 0)

    wo_copies = [
        remote(out_ssm, wo.at[c, 1], wo_sem.at[0], wo_sem.at[1], {"tp": other}),
        remote(out_attn, wo.at[c, 0], wo_sem.at[2], wo_sem.at[3], {"tp": other}),
    ]

    def exchange(src, dst, send, recv, j):
        to, r = 2 * c + j // 2, j % 2
        mine = jnp.logical_and(to == z, c == r)

        @pl.when(mine)
        def _():
            pltpu.make_async_copy(src.at[j], dst, recv.at[z]).start()

        @pl.when(jnp.logical_not(mine))
        def _():
            remote(src.at[j], dst, send.at[j], recv.at[z], {"sp_0": to, "tp": r}).start()

    loads[1].wait()
    loads[2].wait()
    for i in range(2):
        lanes = slice(i * PAIR, (i + 1) * PAIR)
        keys = matmul(normed[...], wk[:, lanes])
        for r in range(2):
            kv_in[2 * i + r, 0] = keys[r * HALF : (r + 1) * HALF].astype(BF16)
        values = matmul(normed[...], wv[:, lanes])
        for r in range(2):
            kv_in[2 * i + r, 1] = values[r * HALF : (r + 1) * HALF].T.astype(BF16)
        for r in range(2):
            exchange(kv_in, kv.at[0, z], zs_send, zs_recv, 2 * i + r)
    for copy in wo_copies:
        copy.start()
    def to_neighbour(slot, zz, new_slot, yy, k):
        return remote(
            kv.at[slot, zz],
            kv.at[new_slot, zz],
            ring_send.at[k],
            kv_recv.at[new_slot, zz],
            {"sp_1": yy},
        )

    def to_partner(slot, zz):
        return remote(
            kv.at[slot, zz],
            kv.at[slot + 1, zz],
            core_send.at[slot // 2, zz],
            kv_recv.at[slot + 1, zz],
            {"tp": other},
        )

    at = [z, lax.rem(z + 1, 2), jnp.where(z < 2, 2, z - 2), jnp.where(z == 3, 2, 3)]

    def serve(t):
        arrived(kv.at[0, at[t]], zs_recv.at[at[t]])
        to_neighbour(0, at[t], 6, right, t).start()
        to_neighbour(0, at[t], 2, left, 4 + t).start()
        to_partner(0, at[t]).start()

    loads[3].wait()
    for i in range(2):
        if i:
            serve(0)
        queries = matmul(normed[...], wq[:, i * PAIR : (i + 1) * PAIR])
        for r in range(2):
            q_in[2 * i + r] = queries[r * HALF : (r + 1) * HALF].T.astype(BF16)
            exchange(q_in, q.at[z], zq_send, zq_recv, 2 * i + r)


    for k in (4, 5, 6):
        loads[k].wait()
    for wide, lanes, at_lane in (
        (wx, slice(0, 256), 0),
        (wx, slice(256, 512), 256),
        (wb, slice(0, 256), 512),
        (wc, slice(0, 256), 768),
    ):
        part = matmul(normed[...], wide[:, lanes]).astype(BF16)
        pre[8:520, at_lane : at_lane + 256] = part.astype(F32)
        halo_out[:, at_lane : at_lane + 256] = part[496:512]
    halo_copy = remote(
        halo_out, halo_in, halo_sem.at[0], halo_sem.at[1], {"sp_0": next_z, "sp_1": right}
    )
    halo_copy.start()
    loads[7].wait()
    for i in range(2):
        lanes = slice(i * 256, (i + 1) * 256)
        gate[:, lanes] = matmul(normed[...], wg[:, lanes]).astype(BF16)
    loads[8].wait()
    narrow[...] = contract(ws[...], normed[...], 1, 1).astype(BF16).astype(F32)

    def convolve(blocks):
        for at_lane, (taps, lanes) in enumerate(
            (
                (conv_inner, slice(0, 256)),
                (conv_inner, slice(256, 512)),
                (conv_bvec, slice(0, 256)),
                (conv_cvec, slice(0, 256)),
            )
        ):
            here = slice(at_lane * 256, at_lane * 256 + 256)
            weight = taps[:, lanes].astype(F32)
            for n in blocks:
                first = 5 + n * BLOCK
                summed = pre[first : first + BLOCK, here] * weight[0:1]
                for o in range(1, 4):
                    summed = summed + pre[first + o : first + o + BLOCK, here] * weight[o : o + 1]
                act[n * BLOCK : (n + 1) * BLOCK, here] = (
                    summed * jax.nn.sigmoid(summed)
                ).astype(BF16)

    convolve((1, 2, 3))
    arrived(halo_in, halo_sem.at[1])
    begins = jnp.logical_and(z == 0, y == 0)
    pre[0:8, :] = halo_in[...].astype(F32)[8:16] * jnp.where(begins, 0.0, 1.0)
    convolve((0,))

    rate = jnp.zeros((8, 128), F32)
    sub = lax.broadcasted_iota(jnp.int32, (8, 128), 0)
    lane8 = lax.broadcasted_iota(jnp.int32, (8, 128), 1)
    for h in range(8):
        rate = jnp.where(sub == h, a_log[0, h], rate)
    rate = -jnp.exp(rate)
    t_at = lax.broadcasted_iota(jnp.int32, (BLOCK, BLOCK), 0)
    s_at = lax.broadcasted_iota(jnp.int32, (BLOCK, BLOCK), 1)
    causal = s_at <= t_at
    low_lane = s_at < SSM_P
    quarter = lax.broadcasted_iota(jnp.int32, (BLOCK, 256), 1) // SSM_P

    def spread(tile, first):
        pairs = [
            jnp.where(low_lane, tile[:, first + a : first + a + 1], tile[:, first + a + 1 : first + a + 2])
            for a in (0, 2)
        ]
        return jnp.concatenate(pairs, axis=1)

    def by_head(tile):
        return jnp.concatenate(
            [jnp.broadcast_to(tile[h : h + 1], (SSM_P, 128)) for h in range(tile.shape[0])], axis=0
        )

    def split_dot(left_side, right_side):
        high = right_side.astype(BF16)
        low = (right_side - high.astype(F32)).astype(BF16)
        return contract(left_side, high, 1, 1) + contract(left_side, low, 1, 1)

    state[...] = jnp.zeros_like(state)
    preceding = jnp.zeros((8, 128), F32)
    for n in range(4):
        rows = slice(n * BLOCK, (n + 1) * BLOCK)
        step_pre = narrow[:, rows]
        decay_row = decay_add[:, rows]
        size = jnp.maximum(step_pre, 0.0) + jnp.log1p(jnp.exp(-jnp.abs(step_pre)))
        running = rate * size + decay_row
        for shift in (1, 2, 4, 8, 16, 32, 64):
            running = running + jnp.where(lane8 >= shift, pltpu.roll(running, shift, 1), 0.0)
        last = jnp.broadcast_to(running[:, 127:128], (8, 128))
        to_end = jnp.exp(last - running) * size
        tall = jnp.concatenate(
            [running, to_end, jnp.exp(running), jnp.exp(running + preceding), jnp.zeros((96, 128), F32)],
            axis=0,
        ).T
        cols[rows, :] = tall
        keep = jnp.exp(last)
        preceding = preceding + last
        for g in range(2):
            lanes = slice(g * 256, (g + 1) * 256)
            inputs_x = act[rows, lanes]
            inputs_b = act[rows, 512 + g * 128 : 640 + g * 128]
            inputs_c = act[rows, 768 + g * 128 : 896 + g * 128]
            crossing = contract(inputs_c, inputs_b, 1, 1)
            mixes, own_x = [], []
            for a in range(4):
                h = 4 * g + a
                fade = jnp.exp(
                    jnp.where(causal, tall[:, h : h + 1] - running[h : h + 1, :], NEG)
                )
                mixes.append((crossing * fade * size[h : h + 1, :]).astype(BF16))
                own_x.append(jnp.where(quarter == a, inputs_x, jnp.zeros_like(inputs_x)))
            inside = matmul(jnp.concatenate(mixes, axis=1), jnp.concatenate(own_x, axis=0))
            weighted = (inputs_x.astype(F32) * spread(tall, 8 + 4 * g)).astype(BF16)
            fresh = contract(weighted, inputs_b, 0, 0)
            before = state[lanes, :]
            carried = split_dot(inputs_c, before) * spread(tall, 16 + 4 * g)
            ysum[rows, lanes] = inside + carried
            state[lanes, :] = before * by_head(keep[4 * g : 4 * g + 4]) + fresh
        if n == 0:
            serve(1)
    for j in range(4):
        st_out[j] = state[j * 128 : (j + 1) * 128, :].astype(BF16)
        tot_out[j] = jnp.concatenate(
            [jnp.broadcast_to(preceding[2 * j + e : 2 * j + e + 1], (4, 128)) for e in range(2)], axis=0
        )
    st_y[y] = st_out[y]
    tot_y[y] = tot_out[y]
    for dy in range(1, 4):
        yy = lax.rem(y + dy, 4)
        remote(st_out.at[yy], st_y.at[y], sty_send.at[0, yy], sty_recv.at[0, y], {"sp_1": yy}).start()
        remote(tot_out.at[yy], tot_y.at[y], sty_send.at[1, yy], sty_recv.at[1, y], {"sp_1": yy}).start()

    serve(2)
    serve(3)

    def wait_chunk(slot, zz):
        arrived(kv.at[slot, zz], kv_recv.at[slot, zz])

    def unit(zqs, pair, zc, masked):
        parts = []
        for zq in zqs:
            for m in range(2):
                lanes = slice(m * QK_DIM, (m + 1) * QK_DIM)
                queries = q[zq, lanes, :]
                scores = [matmul(kv[2 * pair + e, zc, 0, :, lanes], queries) for e in range(2)]
                if masked:
                    key_at = lax.broadcasted_iota(jnp.int32, scores[0].shape, 0)
                    query_at = lax.broadcasted_iota(jnp.int32, scores[0].shape, 1)
                    scores = [
                        jnp.where(key_at <= query_at, scores[0], NEG),
                        jnp.where(key_at <= query_at + (2 * c - 1) * HALF, scores[1], NEG),
                    ]
                parts.append((zq, m, scores, peak[zq, m], total[zq, m]))
        ready = []
        for zq, m, scores, old, sums in parts:
            top = jnp.maximum(
                jnp.max(scores[0], axis=0, keepdims=True), jnp.max(scores[1], axis=0, keepdims=True)
            )
            new = jnp.maximum(old, top * SCALE2)
            weights = [jnp.exp2(part * SCALE2 - new[0:1]) for part in scores]
            shrink = jnp.exp2(old - new)
            sums = sums * shrink + (
                jnp.sum(weights[0], axis=0, keepdims=True) + jnp.sum(weights[1], axis=0, keepdims=True)
            )
            value = matmul(kv[2 * pair, zc, 1], weights[0].astype(BF16)) + matmul(
                kv[2 * pair + 1, zc, 1], weights[1].astype(BF16)
            )
            ready.append((zq, m, new, sums, acc[zq, m] * shrink[0:1] + value))
        for zq, m, new, sums, value in ready:
            peak[zq, m] = new
            total[zq, m] = sums
            acc[zq, m] = value

    def over(pair, zc, low):
        def two(k, carry):
            unit([3 - 2 * k, 2 - 2 * k], pair, zc, False)
            return carry

        lax.fori_loop(0, (4 - low) // 2, two, 0)

        @pl.when(lax.rem(low, 2) == 1)
        def _():
            unit([low], pair, zc, False)
    def two_heads(tile):
        tile = jnp.exp(tile)
        return jnp.concatenate(
            [jnp.broadcast_to(tile[4 * e : 4 * e + 1], (SSM_P, 128)) for e in range(2)], axis=0
        )

    def take(t):
        wait_chunk(6, at[t])
        if t < 2:
            to_neighbour(6, at[t], 4, right, 8 + t).start()
        to_partner(6, at[t]).start()
        wait_chunk(2, at[t])
        if t >= 2:
            to_neighbour(2, at[t], 4, left, 8 + t).start()
        to_partner(2, at[t]).start()

    take(0)
    for t in range(4):
        arrived(q.at[at[t]], zq_recv.at[at[t]])

    def own_chunk(t, carry):
        zc = jnp.where(t == 0, at[0], jnp.where(t == 1, at[1], jnp.where(t == 2, at[2], at[3])))
        wait_chunk(1, zc)
        unit([zc], 0, zc, True)
        over(0, zc, zc + 1)
        return carry

    lax.fori_loop(0, 4, own_chunk, 0)

    def row_prefix():
        for dy in range(1, 4):
            yy = lax.rem(y + dy, 4)
            arrived(st_y.at[yy], sty_recv.at[0, yy])
            arrived(tot_y.at[yy], sty_recv.at[1, yy])
        run_s, run_t = jnp.zeros((128, 128), F32), jnp.zeros((8, 128), F32)
        for k in range(4):
            pre_s[k] = run_s
            pre_t[k] = run_t
            run_s = run_s * two_heads(tot_y[k]) + st_y[k].astype(F32)
            run_t = run_t + tot_y[k]
        row_out[...] = run_s.astype(BF16)
        rtot_out[...] = run_t
        st_z[z] = run_s.astype(BF16)
        tot_z[z] = run_t
        for dz in range(1, 4):
            where = {"sp_0": lax.rem(z + dz, 4)}
            remote(row_out, st_z.at[z], stz_send.at[0, dz], stz_recv.at[0, z], where).start()
            remote(rtot_out, tot_z.at[z], stz_send.at[1, dz], stz_recv.at[1, z], where).start()

    def far_prefix():
        for dz in range(1, 4):
            zz = lax.rem(z + dz, 4)
            arrived(st_z.at[zz], stz_recv.at[0, zz])
            arrived(tot_z.at[zz], stz_recv.at[1, zz])
        run = jnp.zeros((128, 128), F32)
        for k in range(3):
            run = jnp.where(k < z, run * two_heads(tot_z[k]) + st_z[k].astype(F32), run)
        for k in range(4):
            inc_out[k] = (run * two_heads(pre_t[k]) + pre_s[k]).astype(BF16)
        inc_in[y] = inc_out[y]
        for dy in range(1, 4):
            yy = lax.rem(y + dy, 4)
            remote(inc_out.at[yy], inc_in.at[y], inc_send.at[yy], inc_recv.at[y], {"sp_1": yy}).start()

    def finish_ssm():
        for dy in range(1, 4):
            yy = lax.rem(y + dy, 4)
            arrived(inc_in.at[yy], inc_recv.at[yy])
        came = [jnp.concatenate([inc_in[2 * g], inc_in[2 * g + 1]], axis=0) for g in range(2)]
        for n in range(4):
            rows = slice(n * BLOCK, (n + 1) * BLOCK)
            for g in range(2):
                lanes = slice(g * 256, (g + 1) * 256)
                inputs_c = act[rows, 768 + g * 128 : 896 + g * 128]
                value = ysum[rows, lanes] + contract(inputs_c, came[g], 1, 1) * spread(
                    cols[rows, :], 24 + 4 * g
                )
                opened = gate[rows, lanes].astype(F32)
                value = value * (opened * jax.nn.sigmoid(opened))
                scale = lax.rsqrt(jnp.mean(value * value, axis=1, keepdims=True) + EPS)
                ssm_all[n // 2, (n % 2) * BLOCK : (n % 2 + 1) * BLOCK, lanes] = (
                    value * scale * ssm_gain[:, lanes]
                ).astype(BF16)
        ssm_buf[c] = ssm_all[c]
        remote(ssm_all.at[other], ssm_buf.at[c], ssm_sem.at[0], ssm_sem.at[1], {"tp": other}).start()

    def project_ssm():
        arrived(ssm_buf.at[other], ssm_sem.at[1])
        loads[9].wait()
        arrived(wo.at[other, 1], wo_sem.at[1])
        for k in range(4):
            lanes = slice(k * 512, (k + 1) * 512)
            joined[:, lanes] = matmul(ssm_buf[0], wo[0, 1, :, lanes]) + matmul(
                ssm_buf[1], wo[1, 1, :, lanes]
            )

    def finish(zq, carry):
        differ = acc[zq, 0] / total[zq, 0, 0:1] - lam * (acc[zq, 1] / total[zq, 1, 0:1])
        scale = lax.rsqrt(jnp.mean(differ * differ, axis=0, keepdims=True) + EPS)
        done_out[zq] = (differ * scale * gain_col[...]).astype(BF16)

        @pl.when(zq == z)
        def _():
            pltpu.make_async_copy(done_out.at[zq], back.at[z], back_recv.at[z]).start()

        @pl.when(zq != z)
        def _():
            remote(
                done_out.at[zq], back.at[z], back_send.at[zq], back_recv.at[z], {"sp_0": zq}
            ).start()

        return carry

    def later(pair, zc):
        return zc + jnp.where(lax.rem(y + pair, 4) > y, 1, 0)

    def near(t):
        def side(k, carry):
            pair = 3 - 2 * k
            wait_chunk(2 * pair + 1, at[t])
            over(pair, at[t], later(pair, at[t]))
            return carry

        lax.fori_loop(0, 2, side, 0)

    def take_far(t):
        wait_chunk(4, at[t])
        to_partner(4, at[t]).start()

    def far(t):
        wait_chunk(5, at[t])
        over(2, at[t], later(2, at[t]))

    row_prefix()
    take(1)
    near(0)
    take(2)
    far_prefix()
    near(1)
    take(3)
    near(2)
    take_far(0)
    near(3)
    far(0)
    take_far(1)
    finish_ssm()
    project_ssm()
    take_far(2)
    far(1)
    far(2)
    arrived(lam_in, lam_sem.at[1])
    held = jnp.where(z // 2 == c, lam_own[lax.rem(z, 2)], lam_in[lax.rem(z, 2)])
    lam = jnp.concatenate([held, held], axis=1)[0:1]
    gain_col[...] = jnp.broadcast_to(head_gain[...], (PAIR, PAIR)).T
    lax.fori_loop(0, at[3], finish, 0)
    take_far(3)
    far(3)
    lax.fori_loop(at[3], 4, finish, 0)
    out_copies = []
    loads[10].wait()
    arrived(wo.at[other, 0], wo_sem.at[3])
    for k, h in enumerate((z, lax.rem(z + 3, 4), lax.rem(z + 1, 4), lax.rem(z + 2, 4))):
        arrived(back.at[h], back_recv.at[h])
        weight = wo.at[h // 2, 0, pl.ds(pl.multiple_of(lax.rem(h, 2) * PAIR, PAIR), PAIR)]
        for n in range(4):
            lanes = slice(n * 512, (n + 1) * 512)
            sum_n = joined[:, lanes] + contract(back[h], weight[:, lanes], 0, 0)
            if k < 3:
                joined[:, lanes] = sum_n
            else:
                result[:, lanes] = sum_n.astype(BF16)
                out_copies.append(
                    pltpu.make_async_copy(
                        result.at[:, lanes], out_ref.at[:, lanes], out_sem.at[n]
                    )
                )
                out_copies[-1].start()

    x_copy.wait_send()
    lam_copy.wait_send()
    halo_copy.wait_send()
    for copy in wo_copies:
        copy.wait_send()
    for j in range(4):
        mine = jnp.logical_and(2 * c + j // 2 == z, c == j % 2)

        @pl.when(jnp.logical_not(mine))
        def _():
            arrived(kv_in.at[j], zs_send.at[j])
            arrived(q_in.at[j], zq_send.at[j])

    for k in range(12):
        arrived(kv.at[0, 0], ring_send.at[k])
    for s in range(4):
        for t in range(4):
            arrived(kv.at[0, 0], core_send.at[s, t])
    for d in range(1, 4):
        yy = lax.rem(y + d, 4)
        arrived(st_out.at[yy], sty_send.at[0, yy])
        arrived(tot_out.at[yy], sty_send.at[1, yy])
        arrived(inc_out.at[yy], inc_send.at[yy])
        arrived(row_out, stz_send.at[0, d])
        arrived(rtot_out, stz_send.at[1, d])
    arrived(ssm_all.at[0], ssm_sem.at[0])
    for d in range(1, 4):
        arrived(done_out.at[0], back_send.at[lax.rem(z + d, 4)])
    for copy in out_copies:
        copy.wait()


def per_device(
    hidden_in,
    in_gain,
    w_query,
    w_key,
    w_value,
    w_gate,
    w_inner,
    w_bvec,
    w_cvec,
    w_step,
    conv_inner,
    conv_bvec,
    conv_cvec,
    a_log,
    decay_add,
    lambdas,
    head_gain,
    ssm_gain,
    out_attn,
    out_ssm,
):
    vmem = pl.BlockSpec(memory_space=pltpu.VMEM)
    smem = pl.BlockSpec(memory_space=pltpu.SMEM)
    away = pl.BlockSpec(memory_space=pl.ANY)
    dma = pltpu.SemaphoreType.DMA
    buf = pltpu.VMEM
    return pl.pallas_call(
        layer_kernel,
        out_shape=jax.ShapeDtypeStruct((HALF, D), BF16),
        in_specs=[away, vmem]
        + [away] * 8
        + [vmem] * 3
        + [smem, vmem, smem, vmem, vmem, away, away],
        out_specs=away,
        scratch_shapes=[
            buf((2, ROWS, 1024), BF16),
            buf((ROWS, D), BF16),
            buf((D, 512), BF16),
            buf((D, 512), BF16),
            buf((D, 512), BF16),
            buf((D, 512), BF16),
            buf((D, 512), BF16),
            buf((D, 256), BF16),
            buf((D, 256), BF16),
            buf((8, D), BF16),
            buf((2, 2, 512, D), BF16),
            buf((4, 2, HALF, PAIR), BF16),
            buf((4, PAIR, HALF), BF16),
            buf((8, 4, 2, HALF, PAIR), BF16),
            buf((4, PAIR, HALF), BF16),
            buf((4, 2, PAIR, HALF), F32),
            buf((4, 2, 8, HALF), F32),
            buf((4, 2, 8, HALF), F32),
            buf((4, PAIR, HALF), BF16),
            buf((4, PAIR, HALF), BF16),
            buf((520, 1024), F32),
            buf((16, 1024), BF16),
            buf((16, 1024), BF16),
            buf((ROWS, 1024), BF16),
            buf((ROWS, 512), BF16),
            buf((8, ROWS), F32),
            buf((ROWS, 128), F32),
            buf((ROWS, 512), F32),
            buf((512, 128), F32),
            buf((4, 128, 128), BF16),
            buf((4, 8, 128), F32),
            buf((4, 128, 128), BF16),
            buf((4, 8, 128), F32),
            buf((128, 128), BF16),
            buf((8, 128), F32),
            buf((4, 128, 128), BF16),
            buf((4, 8, 128), F32),
            buf((4, 128, 128), F32),
            buf((4, 8, 128), F32),
            buf((4, 128, 128), BF16),
            buf((4, 128, 128), BF16),
            buf((2, HALF, 512), BF16),
            buf((2, HALF, 512), BF16),
            buf((HALF, D), F32),
            buf((2, 8, 128), F32),
            buf((2, 8, 128), F32),
            buf((PAIR, PAIR), F32),
            buf((HALF, D), BF16),
            dma((11,)),
            dma((2,)),
            dma((4,)),
            dma((4,)),
            dma((4,)),
            dma((4,)),
            dma((4,)),
            dma((12,)),
            dma((8, 4)),
            dma((4, 4)),
            dma((4,)),
            dma((4,)),
            dma((2,)),
            dma((2, 4)),
            dma((2, 4)),
            dma((2, 4)),
            dma((2, 4)),
            dma((2,)),
            dma((2,)),
            dma((4,)),
            dma((4,)),
            dma((4,)),
        ],
        compiler_params=pltpu.CompilerParams(
            collective_id=0, has_side_effects=True, vmem_limit_bytes=63 * 2**20
        ),
    )(
        hidden_in,
        in_gain.reshape(1, D),
        w_query,
        w_key,
        w_value,
        w_gate,
        w_inner,
        w_bvec,
        w_cvec,
        w_step.T,
        conv_inner,
        conv_bvec,
        conv_cvec,
        a_log.reshape(1, 8),
        decay_add.T,
        lambdas.reshape(1, 2),
        head_gain.reshape(1, PAIR),
        ssm_gain.reshape(1, 512),
        out_attn,
        out_ssm,
    )


def solution(mesh):
    split = Mesh(
        mesh.devices.reshape(4, 4, mesh.shape["fs"], mesh.shape["tp"]), ("sp_0", "sp_1", "fs", "tp")
    )
    in_specs = (
        P(FS_SP, "tp"),
        P(),
        P(None, "tp"),
        P(None, "tp"),
        P(None, "tp"),
        P(None, "tp"),
        P(None, "tp"),
        P(None, "tp"),
        P(None, "tp"),
        P(None, "tp"),
        P(None, "tp"),
        P(None, "tp"),
        P(None, "tp"),
        P("tp"),
        P(FS_SP, "tp"),
        P("tp"),
        P(),
        P("tp"),
        P("tp", None),
        P("tp", None),
    )
    out_specs = P(FS_SP_TP, None)
    return jax.shard_map(
        per_device, mesh=split, in_specs=in_specs, out_specs=out_specs, check_vma=False
    )
```

```python
import jax
import jax.numpy as jnp
from jax import lax
from jax.experimental import pallas as pl
from jax.experimental.pallas import tpu as pltpu
from jax.sharding import Mesh
from jax.sharding import PartitionSpec as P

D = 2048
QK_DIM = 128
SSM_P = 64
STATE = 128
BLOCK = 128
ROWS = 512
HALF = 256
PAIR = 256
FS_SP = ("fs", "sp_0", "sp_1")
FS_SP_TP = ("fs", "sp_0", "sp_1", "tp")
MESH = pl.DeviceIdType.MESH
SCALE2 = QK_DIM ** (-0.5) * 1.4426950408889634
EPS = 1e-06
NEG = -1e30
F32, BF16 = jnp.float32, jnp.bfloat16


def matmul(a, b):
    return jnp.dot(a, b, preferred_element_type=F32)


def contract(a, b, da, db):
    return lax.dot_general(a, b, (((da,), (db,)), ((), ())), preferred_element_type=F32)


def arrived(ref, sem):
    pltpu.make_async_copy(ref, ref, sem).wait()


def layer_kernel(
    hidden,
    in_gain,
    w_query,
    w_key,
    w_value,
    w_gate,
    w_inner,
    w_bvec,
    w_cvec,
    w_step,
    conv_inner,
    conv_bvec,
    conv_cvec,
    a_log,
    decay_add,
    lambdas,
    head_gain,
    ssm_gain,
    out_attn,
    out_ssm,
    out_ref,
    x,
    normed,
    wq,
    wk,
    wv,
    wg,
    wx,
    wb,
    wc,
    ws,
    wo,
    kv_in,
    q_in,
    kv,
    q,
    acc,
    peak,
    total,
    done_out,
    back,
    pre,
    halo_out,
    halo_in,
    act,
    gate,
    narrow,
    cols,
    ysum,
    state,
    st_out,
    tot_out,
    st_y,
    tot_y,
    row_out,
    rtot_out,
    st_z,
    tot_z,
    pre_s,
    pre_t,
    inc_out,
    inc_in,
    ssm_all,
    ssm_buf,
    joined,
    lam_own,
    lam_in,
    gain_col,
    result,
    load_sem,
    x_sem,
    wo_sem,
    zs_send,
    zs_recv,
    zq_send,
    zq_recv,
    ring_send,
    kv_recv,
    core_send,
    back_send,
    back_recv,
    halo_sem,
    sty_send,
    sty_recv,
    stz_send,
    stz_recv,
    ssm_sem,
    lam_sem,
    out_sem,
    inc_send,
    inc_recv,
):
    z, y, c = lax.axis_index("sp_0"), lax.axis_index("sp_1"), lax.axis_index("tp")
    right, left = lax.rem(y + 1, 4), lax.rem(y + 3, 4)
    other = 1 - c
    next_z = lax.rem(z + jnp.where(y == 3, 1, 0), 4)
    prev_z = lax.rem(z + jnp.where(y == 0, 3, 0), 4)

    loads = []
    for k, (src, dst) in enumerate(
        (
            (hidden, x.at[c]),
            (w_key, wk),
            (w_value, wv),
            (w_query, wq),
            (w_inner, wx),
            (w_bvec, wb),
            (w_cvec, wc),
            (w_gate, wg),
            (w_step, ws),
            (out_ssm, wo.at[c, 1]),
            (out_attn, wo.at[c, 0]),
        )
    ):
        loads.append(pltpu.make_async_copy(src, dst, load_sem.at[k]))
        loads[-1].start()

    barrier = pltpu.get_barrier_semaphore()

    def greet(where):
        pl.semaphore_signal(barrier, inc=1, device_id=where, device_id_type=MESH)

    for dz in range(4):
        for dc in range(2):
            if dz or dc:
                greet({"sp_0": lax.rem(z + dz, 4), "tp": lax.rem(c + dc, 2)})
    for dy in range(1, 4):
        greet({"sp_1": lax.rem(y + dy, 4)})
    greet({"sp_0": next_z, "sp_1": right})
    greet({"sp_0": prev_z, "sp_1": left})
    pl.semaphore_wait(barrier, 12)

    def remote(src, dst, send, recv, where):
        return pltpu.make_async_remote_copy(
            src_ref=src,
            dst_ref=dst,
            send_sem=send,
            recv_sem=recv,
            device_id=where,
            device_id_type=MESH,
        )

    x_copy = remote(hidden, x.at[c], x_sem.at[0], x_sem.at[1], {"tp": other})
    x_copy.start()

    acc[...] = jnp.zeros_like(acc)
    total[...] = jnp.zeros_like(total)
    peak[...] = jnp.full_like(peak, NEG)
    for i in range(2):
        lam_own[i] = jnp.full((8, 128), lambdas[0, i], F32)
    lam_copy = remote(lam_own, lam_in, lam_sem.at[0], lam_sem.at[1], {"tp": other})
    lam_copy.start()

    loads[0].wait()
    arrived(x.at[other], x_sem.at[1])

    def norm_rows(n, carry):
        rows = pl.ds(pl.multiple_of(n * 64, 64), 64)
        first, second = x[0, rows, :].astype(F32), x[1, rows, :].astype(F32)
        squares = jnp.sum(first * first, axis=1, keepdims=True) + jnp.sum(
            second * second, axis=1, keepdims=True
        )
        scale = lax.rsqrt(squares / D + EPS)
        normed[rows, 0:1024] = (first * scale * in_gain[:, 0:1024]).astype(BF16)
        normed[rows, 1024:2048] = (second * scale * in_gain[:, 1024:2048]).astype(BF16)
        return carry

    lax.fori_loop(0, 8, norm_rows, 0)

    wo_copies = [
        remote(out_ssm, wo.at[c, 1], wo_sem.at[0], wo_sem.at[1], {"tp": other}),
        remote(out_attn, wo.at[c, 0], wo_sem.at[2], wo_sem.at[3], {"tp": other}),
    ]

    def exchange(src, dst, send, recv, j):
        to, r = 2 * c + j // 2, j % 2
        mine = jnp.logical_and(to == z, c == r)

        @pl.when(mine)
        def _():
            pltpu.make_async_copy(src.at[j], dst, recv.at[z]).start()

        @pl.when(jnp.logical_not(mine))
        def _():
            remote(src.at[j], dst, send.at[j], recv.at[z], {"sp_0": to, "tp": r}).start()

    loads[1].wait()
    loads[2].wait()
    for i in range(2):
        lanes = slice(i * PAIR, (i + 1) * PAIR)
        keys = matmul(normed[...], wk[:, lanes])
        for r in range(2):
            kv_in[2 * i + r, 0] = keys[r * HALF : (r + 1) * HALF].astype(BF16)
        values = matmul(normed[...], wv[:, lanes])
        for r in range(2):
            kv_in[2 * i + r, 1] = values[r * HALF : (r + 1) * HALF].T.astype(BF16)
        for r in range(2):
            exchange(kv_in, kv.at[0, z], zs_send, zs_recv, 2 * i + r)
    for copy in wo_copies:
        copy.start()
    def to_neighbour(slot, zz, new_slot, yy, k):
        return remote(
            kv.at[slot, zz],
            kv.at[new_slot, zz],
            ring_send.at[k],
            kv_recv.at[new_slot, zz],
            {"sp_1": yy},
        )

    def to_partner(slot, zz):
        return remote(
            kv.at[slot, zz],
            kv.at[slot + 1, zz],
            core_send.at[slot // 2, zz],
            kv_recv.at[slot + 1, zz],
            {"tp": other},
        )

    at = [z, lax.rem(z + 1, 2), jnp.where(z < 2, 2, z - 2), jnp.where(z == 3, 2, 3)]

    def serve(t):
        arrived(kv.at[0, at[t]], zs_recv.at[at[t]])
        to_neighbour(0, at[t], 6, right, t).start()
        to_neighbour(0, at[t], 2, left, 4 + t).start()
        to_partner(0, at[t]).start()

    loads[3].wait()
    for i in range(2):
        if i:
            serve(0)
        queries = matmul(normed[...], wq[:, i * PAIR : (i + 1) * PAIR])
        for r in range(2):
            q_in[2 * i + r] = queries[r * HALF : (r + 1) * HALF].T.astype(BF16)
            exchange(q_in, q.at[z], zq_send, zq_recv, 2 * i + r)


    for k in (4, 5, 6):
        loads[k].wait()
    for wide, lanes, at_lane in (
        (wx, slice(0, 256), 0),
        (wx, slice(256, 512), 256),
        (wb, slice(0, 256), 512),
        (wc, slice(0, 256), 768),
    ):
        part = matmul(normed[...], wide[:, lanes]).astype(BF16)
        pre[8:520, at_lane : at_lane + 256] = part.astype(F32)
        halo_out[:, at_lane : at_lane + 256] = part[496:512]
    halo_copy = remote(
        halo_out, halo_in, halo_sem.at[0], halo_sem.at[1], {"sp_0": next_z, "sp_1": right}
    )
    halo_copy.start()
    loads[7].wait()
    for i in range(2):
        lanes = slice(i * 256, (i + 1) * 256)
        gate[:, lanes] = matmul(normed[...], wg[:, lanes]).astype(BF16)
    loads[8].wait()
    narrow[...] = contract(ws[...], normed[...], 1, 1).astype(BF16).astype(F32)

    def convolve(blocks):
        for at_lane, (taps, lanes) in enumerate(
            (
                (conv_inner, slice(0, 256)),
                (conv_inner, slice(256, 512)),
                (conv_bvec, slice(0, 256)),
                (conv_cvec, slice(0, 256)),
            )
        ):
            here = slice(at_lane * 256, at_lane * 256 + 256)
            weight = taps[:, lanes].astype(F32)
            for n in blocks:
                first = 5 + n * BLOCK
                summed = pre[first : first + BLOCK, here] * weight[0:1]
                for o in range(1, 4):
                    summed = summed + pre[first + o : first + o + BLOCK, here] * weight[o : o + 1]
                act[n * BLOCK : (n + 1) * BLOCK, here] = (
                    summed * jax.nn.sigmoid(summed)
                ).astype(BF16)

    convolve((1, 2, 3))
    arrived(halo_in, halo_sem.at[1])
    begins = jnp.logical_and(z == 0, y == 0)
    pre[0:8, :] = halo_in[...].astype(F32)[8:16] * jnp.where(begins, 0.0, 1.0)
    convolve((0,))

    rate = jnp.zeros((8, 128), F32)
    sub = lax.broadcasted_iota(jnp.int32, (8, 128), 0)
    lane8 = lax.broadcasted_iota(jnp.int32, (8, 128), 1)
    for h in range(8):
        rate = jnp.where(sub == h, a_log[0, h], rate)
    rate = -jnp.exp(rate)
    t_at = lax.broadcasted_iota(jnp.int32, (BLOCK, BLOCK), 0)
    s_at = lax.broadcasted_iota(jnp.int32, (BLOCK, BLOCK), 1)
    causal = s_at <= t_at
    low_lane = s_at < SSM_P
    quarter = lax.broadcasted_iota(jnp.int32, (BLOCK, 256), 1) // SSM_P

    def spread(tile, first):
        pairs = [
            jnp.where(low_lane, tile[:, first + a : first + a + 1], tile[:, first + a + 1 : first + a + 2])
            for a in (0, 2)
        ]
        return jnp.concatenate(pairs, axis=1)

    def by_head(tile):
        return jnp.concatenate(
            [jnp.broadcast_to(tile[h : h + 1], (SSM_P, 128)) for h in range(tile.shape[0])], axis=0
        )

    def split_dot(left_side, right_side):
        high = right_side.astype(BF16)
        low = (right_side - high.astype(F32)).astype(BF16)
        return contract(left_side, high, 1, 1) + contract(left_side, low, 1, 1)

    state[...] = jnp.zeros_like(state)
    preceding = jnp.zeros((8, 128), F32)
    for n in range(4):
        rows = slice(n * BLOCK, (n + 1) * BLOCK)
        step_pre = narrow[:, rows]
        decay_row = decay_add[:, rows]
        size = jnp.maximum(step_pre, 0.0) + jnp.log1p(jnp.exp(-jnp.abs(step_pre)))
        running = rate * size + decay_row
        for shift in (1, 2, 4, 8, 16, 32, 64):
            running = running + jnp.where(lane8 >= shift, pltpu.roll(running, shift, 1), 0.0)
        last = jnp.broadcast_to(running[:, 127:128], (8, 128))
        to_end = jnp.exp(last - running) * size
        tall = jnp.concatenate(
            [running, to_end, jnp.exp(running), jnp.exp(running + preceding), jnp.zeros((96, 128), F32)],
            axis=0,
        ).T
        cols[rows, :] = tall
        keep = jnp.exp(last)
        preceding = preceding + last
        for g in range(2):
            lanes = slice(g * 256, (g + 1) * 256)
            inputs_x = act[rows, lanes]
            inputs_b = act[rows, 512 + g * 128 : 640 + g * 128]
            inputs_c = act[rows, 768 + g * 128 : 896 + g * 128]
            crossing = contract(inputs_c, inputs_b, 1, 1)
            mixes, own_x = [], []
            for a in range(4):
                h = 4 * g + a
                fade = jnp.exp(
                    jnp.where(causal, tall[:, h : h + 1] - running[h : h + 1, :], NEG)
                )
                mixes.append((crossing * fade * size[h : h + 1, :]).astype(BF16))
                own_x.append(jnp.where(quarter == a, inputs_x, jnp.zeros_like(inputs_x)))
            inside = matmul(jnp.concatenate(mixes, axis=1), jnp.concatenate(own_x, axis=0))
            weighted = (inputs_x.astype(F32) * spread(tall, 8 + 4 * g)).astype(BF16)
            fresh = contract(weighted, inputs_b, 0, 0)
            before = state[lanes, :]
            carried = split_dot(inputs_c, before) * spread(tall, 16 + 4 * g)
            ysum[rows, lanes] = inside + carried
            state[lanes, :] = before * by_head(keep[4 * g : 4 * g + 4]) + fresh
        if n == 0:
            serve(1)
    for j in range(4):
        st_out[j] = state[j * 128 : (j + 1) * 128, :].astype(BF16)
        tot_out[j] = jnp.concatenate(
            [jnp.broadcast_to(preceding[2 * j + e : 2 * j + e + 1], (4, 128)) for e in range(2)], axis=0
        )
    st_y[y] = st_out[y]
    tot_y[y] = tot_out[y]
    for dy in range(1, 4):
        yy = lax.rem(y + dy, 4)
        remote(st_out.at[yy], st_y.at[y], sty_send.at[0, yy], sty_recv.at[0, y], {"sp_1": yy}).start()
        remote(tot_out.at[yy], tot_y.at[y], sty_send.at[1, yy], sty_recv.at[1, y], {"sp_1": yy}).start()

    serve(2)
    serve(3)

    def wait_chunk(slot, zz):
        arrived(kv.at[slot, zz], kv_recv.at[slot, zz])

    def unit(zqs, pair, zc, masked):
        parts = []
        for zq in zqs:
            for m in range(2):
                lanes = slice(m * QK_DIM, (m + 1) * QK_DIM)
                queries = q[zq, lanes, :]
                scores = [matmul(kv[2 * pair + e, zc, 0, :, lanes], queries) for e in range(2)]
                if masked:
                    key_at = lax.broadcasted_iota(jnp.int32, scores[0].shape, 0)
                    query_at = lax.broadcasted_iota(jnp.int32, scores[0].shape, 1)
                    scores = [
                        jnp.where(key_at <= query_at, scores[0], NEG),
                        jnp.where(key_at <= query_at + (2 * c - 1) * HALF, scores[1], NEG),
                    ]
                parts.append((zq, m, scores, peak[zq, m], total[zq, m]))
        ready = []
        for zq, m, scores, old, sums in parts:
            top = jnp.maximum(
                jnp.max(scores[0], axis=0, keepdims=True), jnp.max(scores[1], axis=0, keepdims=True)
            )
            new = jnp.maximum(old, top * SCALE2)
            weights = [jnp.exp2(part * SCALE2 - new[0:1]) for part in scores]
            shrink = jnp.exp2(old - new)
            sums = sums * shrink + (
                jnp.sum(weights[0], axis=0, keepdims=True) + jnp.sum(weights[1], axis=0, keepdims=True)
            )
            value = matmul(kv[2 * pair, zc, 1], weights[0].astype(BF16)) + matmul(
                kv[2 * pair + 1, zc, 1], weights[1].astype(BF16)
            )
            ready.append((zq, m, new, sums, acc[zq, m] * shrink[0:1] + value))
        for zq, m, new, sums, value in ready:
            peak[zq, m] = new
            total[zq, m] = sums
            acc[zq, m] = value

    def over(pair, zc, low):
        def two(k, carry):
            unit([3 - 2 * k, 2 - 2 * k], pair, zc, False)
            return carry

        lax.fori_loop(0, (4 - low) // 2, two, 0)

        @pl.when(lax.rem(low, 2) == 1)
        def _():
            unit([low], pair, zc, False)
    def two_heads(tile):
        tile = jnp.exp(tile)
        return jnp.concatenate(
            [jnp.broadcast_to(tile[4 * e : 4 * e + 1], (SSM_P, 128)) for e in range(2)], axis=0
        )

    def take(t):
        wait_chunk(6, at[t])
        if t < 2:
            to_neighbour(6, at[t], 4, right, 8 + t).start()
        to_partner(6, at[t]).start()
        wait_chunk(2, at[t])
        if t >= 2:
            to_neighbour(2, at[t], 4, left, 8 + t).start()
        to_partner(2, at[t]).start()

    take(0)
    for t in range(4):
        arrived(q.at[at[t]], zq_recv.at[at[t]])

    def own_chunk(t, carry):
        zc = jnp.where(t == 0, at[0], jnp.where(t == 1, at[1], jnp.where(t == 2, at[2], at[3])))
        wait_chunk(1, zc)
        unit([zc], 0, zc, True)
        over(0, zc, zc + 1)
        return carry

    lax.fori_loop(0, 4, own_chunk, 0)

    def row_prefix():
        for dy in range(1, 4):
            yy = lax.rem(y + dy, 4)
            arrived(st_y.at[yy], sty_recv.at[0, yy])
            arrived(tot_y.at[yy], sty_recv.at[1, yy])
        run_s, run_t = jnp.zeros((128, 128), F32), jnp.zeros((8, 128), F32)
        for k in range(4):
            pre_s[k] = run_s
            pre_t[k] = run_t
            run_s = run_s * two_heads(tot_y[k]) + st_y[k].astype(F32)
            run_t = run_t + tot_y[k]
        row_out[...] = run_s.astype(BF16)
        rtot_out[...] = run_t
        st_z[z] = run_s.astype(BF16)
        tot_z[z] = run_t
        for dz in range(1, 4):
            where = {"sp_0": lax.rem(z + dz, 4)}
            remote(row_out, st_z.at[z], stz_send.at[0, dz], stz_recv.at[0, z], where).start()
            remote(rtot_out, tot_z.at[z], stz_send.at[1, dz], stz_recv.at[1, z], where).start()

    def far_prefix():
        for dz in range(1, 4):
            zz = lax.rem(z + dz, 4)
            arrived(st_z.at[zz], stz_recv.at[0, zz])
            arrived(tot_z.at[zz], stz_recv.at[1, zz])
        run = jnp.zeros((128, 128), F32)
        for k in range(3):
            run = jnp.where(k < z, run * two_heads(tot_z[k]) + st_z[k].astype(F32), run)
        for k in range(4):
            inc_out[k] = (run * two_heads(pre_t[k]) + pre_s[k]).astype(BF16)
        inc_in[y] = inc_out[y]
        for dy in range(1, 4):
            yy = lax.rem(y + dy, 4)
            remote(inc_out.at[yy], inc_in.at[y], inc_send.at[yy], inc_recv.at[y], {"sp_1": yy}).start()

    def finish_ssm():
        for dy in range(1, 4):
            yy = lax.rem(y + dy, 4)
            arrived(inc_in.at[yy], inc_recv.at[yy])
        came = [jnp.concatenate([inc_in[2 * g], inc_in[2 * g + 1]], axis=0) for g in range(2)]
        for n in range(4):
            rows = slice(n * BLOCK, (n + 1) * BLOCK)
            for g in range(2):
                lanes = slice(g * 256, (g + 1) * 256)
                inputs_c = act[rows, 768 + g * 128 : 896 + g * 128]
                value = ysum[rows, lanes] + contract(inputs_c, came[g], 1, 1) * spread(
                    cols[rows, :], 24 + 4 * g
                )
                opened = gate[rows, lanes].astype(F32)
                value = value * (opened * jax.nn.sigmoid(opened))
                scale = lax.rsqrt(jnp.mean(value * value, axis=1, keepdims=True) + EPS)
                ssm_all[n // 2, (n % 2) * BLOCK : (n % 2 + 1) * BLOCK, lanes] = (
                    value * scale * ssm_gain[:, lanes]
                ).astype(BF16)
        ssm_buf[c] = ssm_all[c]
        remote(ssm_all.at[other], ssm_buf.at[c], ssm_sem.at[0], ssm_sem.at[1], {"tp": other}).start()

    def project_ssm():
        arrived(ssm_buf.at[other], ssm_sem.at[1])
        loads[9].wait()
        arrived(wo.at[other, 1], wo_sem.at[1])
        for k in range(4):
            lanes = slice(k * 512, (k + 1) * 512)
            joined[:, lanes] = matmul(ssm_buf[0], wo[0, 1, :, lanes]) + matmul(
                ssm_buf[1], wo[1, 1, :, lanes]
            )

    def finish(zq, carry):
        differ = acc[zq, 0] / total[zq, 0, 0:1] - lam * (acc[zq, 1] / total[zq, 1, 0:1])
        scale = lax.rsqrt(jnp.mean(differ * differ, axis=0, keepdims=True) + EPS)
        done_out[zq] = (differ * scale * gain_col[...]).astype(BF16)

        @pl.when(zq == z)
        def _():
            pltpu.make_async_copy(done_out.at[zq], back.at[z], back_recv.at[z]).start()

        @pl.when(zq != z)
        def _():
            remote(
                done_out.at[zq], back.at[z], back_send.at[zq], back_recv.at[z], {"sp_0": zq}
            ).start()

        return carry

    def later(pair, zc):
        return zc + jnp.where(lax.rem(y + pair, 4) > y, 1, 0)

    def near(t):
        def side(k, carry):
            pair = 3 - 2 * k
            wait_chunk(2 * pair + 1, at[t])
            over(pair, at[t], later(pair, at[t]))
            return carry

        lax.fori_loop(0, 2, side, 0)

    def take_far(t):
        wait_chunk(4, at[t])
        to_partner(4, at[t]).start()

    def far(t):
        wait_chunk(5, at[t])
        over(2, at[t], later(2, at[t]))

    row_prefix()
    take(1)
    near(0)
    take(2)
    far_prefix()
    near(1)
    take(3)
    near(2)
    take_far(0)
    near(3)
    far(0)
    take_far(1)
    finish_ssm()
    take_far(2)
    far(1)
    arrived(lam_in, lam_sem.at[1])
    held = jnp.where(z // 2 == c, lam_own[lax.rem(z, 2)], lam_in[lax.rem(z, 2)])
    lam = jnp.concatenate([held, held], axis=1)[0:1]
    gain_col[...] = jnp.broadcast_to(head_gain[...], (PAIR, PAIR)).T
    whole = jnp.where(z < 2, 2, z - 2)
    lax.fori_loop(0, whole, finish, 0)
    project_ssm()
    take_far(3)
    far(2)
    lax.fori_loop(whole, at[3], finish, 0)
    far(3)
    lax.fori_loop(at[3], 4, finish, 0)
    out_copies = []
    loads[10].wait()
    arrived(wo.at[other, 0], wo_sem.at[3])
    for k, h in enumerate((z, lax.rem(z + 3, 4), lax.rem(z + 1, 4), lax.rem(z + 2, 4))):
        arrived(back.at[h], back_recv.at[h])
        weight = wo.at[h // 2, 0, pl.ds(pl.multiple_of(lax.rem(h, 2) * PAIR, PAIR), PAIR)]
        for n in range(4):
            lanes = slice(n * 512, (n + 1) * 512)
            sum_n = joined[:, lanes] + contract(back[h], weight[:, lanes], 0, 0)
            if k < 3:
                joined[:, lanes] = sum_n
            else:
                result[:, lanes] = sum_n.astype(BF16)
                out_copies.append(
                    pltpu.make_async_copy(
                        result.at[:, lanes], out_ref.at[:, lanes], out_sem.at[n]
                    )
                )
                out_copies[-1].start()

    x_copy.wait_send()
    lam_copy.wait_send()
    halo_copy.wait_send()
    for copy in wo_copies:
        copy.wait_send()
    for j in range(4):
        mine = jnp.logical_and(2 * c + j // 2 == z, c == j % 2)

        @pl.when(jnp.logical_not(mine))
        def _():
            arrived(kv_in.at[j], zs_send.at[j])
            arrived(q_in.at[j], zq_send.at[j])

    for k in range(12):
        arrived(kv.at[0, 0], ring_send.at[k])
    for s in range(4):
        for t in range(4):
            arrived(kv.at[0, 0], core_send.at[s, t])
    for d in range(1, 4):
        yy = lax.rem(y + d, 4)
        arrived(st_out.at[yy], sty_send.at[0, yy])
        arrived(tot_out.at[yy], sty_send.at[1, yy])
        arrived(inc_out.at[yy], inc_send.at[yy])
        arrived(row_out, stz_send.at[0, d])
        arrived(rtot_out, stz_send.at[1, d])
    arrived(ssm_all.at[0], ssm_sem.at[0])
    for d in range(1, 4):
        arrived(done_out.at[0], back_send.at[lax.rem(z + d, 4)])
    for copy in out_copies:
        copy.wait()


def per_device(
    hidden_in,
    in_gain,
    w_query,
    w_key,
    w_value,
    w_gate,
    w_inner,
    w_bvec,
    w_cvec,
    w_step,
    conv_inner,
    conv_bvec,
    conv_cvec,
    a_log,
    decay_add,
    lambdas,
    head_gain,
    ssm_gain,
    out_attn,
    out_ssm,
):
    vmem = pl.BlockSpec(memory_space=pltpu.VMEM)
    smem = pl.BlockSpec(memory_space=pltpu.SMEM)
    away = pl.BlockSpec(memory_space=pl.ANY)
    dma = pltpu.SemaphoreType.DMA
    buf = pltpu.VMEM
    return pl.pallas_call(
        layer_kernel,
        out_shape=jax.ShapeDtypeStruct((HALF, D), BF16),
        in_specs=[away, vmem]
        + [away] * 8
        + [vmem] * 3
        + [smem, vmem, smem, vmem, vmem, away, away],
        out_specs=away,
        scratch_shapes=[
            buf((2, ROWS, 1024), BF16),
            buf((ROWS, D), BF16),
            buf((D, 512), BF16),
            buf((D, 512), BF16),
            buf((D, 512), BF16),
            buf((D, 512), BF16),
            buf((D, 512), BF16),
            buf((D, 256), BF16),
            buf((D, 256), BF16),
            buf((8, D), BF16),
            buf((2, 2, 512, D), BF16),
            buf((4, 2, HALF, PAIR), BF16),
            buf((4, PAIR, HALF), BF16),
            buf((8, 4, 2, HALF, PAIR), BF16),
            buf((4, PAIR, HALF), BF16),
            buf((4, 2, PAIR, HALF), F32),
            buf((4, 2, 8, HALF), F32),
            buf((4, 2, 8, HALF), F32),
            buf((4, PAIR, HALF), BF16),
            buf((4, PAIR, HALF), BF16),
            buf((520, 1024), F32),
            buf((16, 1024), BF16),
            buf((16, 1024), BF16),
            buf((ROWS, 1024), BF16),
            buf((ROWS, 512), BF16),
            buf((8, ROWS), F32),
            buf((ROWS, 128), F32),
            buf((ROWS, 512), F32),
            buf((512, 128), F32),
            buf((4, 128, 128), BF16),
            buf((4, 8, 128), F32),
            buf((4, 128, 128), BF16),
            buf((4, 8, 128), F32),
            buf((128, 128), BF16),
            buf((8, 128), F32),
            buf((4, 128, 128), BF16),
            buf((4, 8, 128), F32),
            buf((4, 128, 128), F32),
            buf((4, 8, 128), F32),
            buf((4, 128, 128), BF16),
            buf((4, 128, 128), BF16),
            buf((2, HALF, 512), BF16),
            buf((2, HALF, 512), BF16),
            buf((HALF, D), F32),
            buf((2, 8, 128), F32),
            buf((2, 8, 128), F32),
            buf((PAIR, PAIR), F32),
            buf((HALF, D), BF16),
            dma((11,)),
            dma((2,)),
            dma((4,)),
            dma((4,)),
            dma((4,)),
            dma((4,)),
            dma((4,)),
            dma((12,)),
            dma((8, 4)),
            dma((4, 4)),
            dma((4,)),
            dma((4,)),
            dma((2,)),
            dma((2, 4)),
            dma((2, 4)),
            dma((2, 4)),
            dma((2, 4)),
            dma((2,)),
            dma((2,)),
            dma((4,)),
            dma((4,)),
            dma((4,)),
        ],
        compiler_params=pltpu.CompilerParams(
            collective_id=0, has_side_effects=True, vmem_limit_bytes=63 * 2**20
        ),
    )(
        hidden_in,
        in_gain.reshape(1, D),
        w_query,
        w_key,
        w_value,
        w_gate,
        w_inner,
        w_bvec,
        w_cvec,
        w_step.T,
        conv_inner,
        conv_bvec,
        conv_cvec,
        a_log.reshape(1, 8),
        decay_add.T,
        lambdas.reshape(1, 2),
        head_gain.reshape(1, PAIR),
        ssm_gain.reshape(1, 512),
        out_attn,
        out_ssm,
    )


def solution(mesh):
    split = Mesh(
        mesh.devices.reshape(4, 4, mesh.shape["fs"], mesh.shape["tp"]), ("sp_0", "sp_1", "fs", "tp")
    )
    in_specs = (
        P(FS_SP, "tp"),
        P(),
        P(None, "tp"),
        P(None, "tp"),
        P(None, "tp"),
        P(None, "tp"),
        P(None, "tp"),
        P(None, "tp"),
        P(None, "tp"),
        P(None, "tp"),
        P(None, "tp"),
        P(None, "tp"),
        P(None, "tp"),
        P("tp"),
        P(FS_SP, "tp"),
        P("tp"),
        P(),
        P("tp"),
        P("tp", None),
        P("tp", None),
    )
    out_specs = P(FS_SP_TP, None)
    return jax.shard_map(
        per_device, mesh=split, in_specs=in_specs, out_specs=out_specs, check_vma=False
    )
```

```python
import jax
import jax.numpy as jnp
from jax import lax
from jax.experimental import pallas as pl
from jax.experimental.pallas import tpu as pltpu
from jax.sharding import Mesh
from jax.sharding import PartitionSpec as P

D = 2048
QK_DIM = 128
SSM_P = 64
STATE = 128
BLOCK = 128
ROWS = 512
HALF = 256
PAIR = 256
FS_SP = ("fs", "sp_0", "sp_1")
FS_SP_TP = ("fs", "sp_0", "sp_1", "tp")
MESH = pl.DeviceIdType.MESH
SCALE2 = QK_DIM ** (-0.5) * 1.4426950408889634
EPS = 1e-06
NEG = -1e30
F32, BF16 = jnp.float32, jnp.bfloat16


def matmul(a, b):
    return jnp.dot(a, b, preferred_element_type=F32)


def contract(a, b, da, db):
    return lax.dot_general(a, b, (((da,), (db,)), ((), ())), preferred_element_type=F32)


def arrived(ref, sem):
    pltpu.make_async_copy(ref, ref, sem).wait()


def layer_kernel(
    hidden,
    in_gain,
    w_query,
    w_key,
    w_value,
    w_gate,
    w_inner,
    w_bvec,
    w_cvec,
    w_step,
    conv_inner,
    conv_bvec,
    conv_cvec,
    a_log,
    decay_add,
    lambdas,
    head_gain,
    ssm_gain,
    out_attn,
    out_ssm,
    out_ref,
    x,
    normed,
    wq,
    wk,
    wv,
    wg,
    wx,
    wb,
    wc,
    ws,
    wo,
    kv_in,
    q_in,
    kv,
    q,
    acc,
    peak,
    total,
    done_out,
    back,
    pre,
    halo_out,
    halo_in,
    act,
    gate,
    narrow,
    cols,
    ysum,
    state,
    st_out,
    tot_out,
    st_y,
    tot_y,
    row_out,
    rtot_out,
    st_z,
    tot_z,
    pre_s,
    pre_t,
    inc_out,
    inc_in,
    ssm_all,
    ssm_buf,
    joined,
    lam_own,
    lam_in,
    gain_col,
    result,
    load_sem,
    x_sem,
    wo_sem,
    zs_send,
    zs_recv,
    zq_send,
    zq_recv,
    ring_send,
    kv_recv,
    core_send,
    back_send,
    back_recv,
    halo_sem,
    sty_send,
    sty_recv,
    stz_send,
    stz_recv,
    ssm_sem,
    lam_sem,
    out_sem,
    inc_send,
    inc_recv,
):
    z, y, c = lax.axis_index("sp_0"), lax.axis_index("sp_1"), lax.axis_index("tp")
    right, left = lax.rem(y + 1, 4), lax.rem(y + 3, 4)
    other = 1 - c
    next_z = lax.rem(z + jnp.where(y == 3, 1, 0), 4)
    prev_z = lax.rem(z + jnp.where(y == 0, 3, 0), 4)

    loads = []
    for k, (src, dst) in enumerate(
        (
            (hidden, x.at[c]),
            (w_key, wk),
            (w_value, wv),
            (w_query, wq),
            (w_inner, wx),
            (w_bvec, wb),
            (w_cvec, wc),
            (w_gate, wg),
            (w_step, ws),
            (out_ssm, wo.at[c, 1]),
            (out_attn, wo.at[c, 0]),
        )
    ):
        loads.append(pltpu.make_async_copy(src, dst, load_sem.at[k]))
        loads[-1].start()

    barrier = pltpu.get_barrier_semaphore()

    def greet(where):
        pl.semaphore_signal(barrier, inc=1, device_id=where, device_id_type=MESH)

    for dz in range(4):
        for dc in range(2):
            if dz or dc:
                greet({"sp_0": lax.rem(z + dz, 4), "tp": lax.rem(c + dc, 2)})
    for dy in range(1, 4):
        greet({"sp_1": lax.rem(y + dy, 4)})
    greet({"sp_0": next_z, "sp_1": right})
    greet({"sp_0": prev_z, "sp_1": left})
    pl.semaphore_wait(barrier, 12)

    def remote(src, dst, send, recv, where):
        return pltpu.make_async_remote_copy(
            src_ref=src,
            dst_ref=dst,
            send_sem=send,
            recv_sem=recv,
            device_id=where,
            device_id_type=MESH,
        )

    x_copy = remote(hidden, x.at[c], x_sem.at[0], x_sem.at[1], {"tp": other})
    x_copy.start()

    acc[...] = jnp.zeros_like(acc)
    total[...] = jnp.zeros_like(total)
    peak[...] = jnp.full_like(peak, NEG)
    for i in range(2):
        lam_own[i] = jnp.full((8, 128), lambdas[0, i], F32)
    lam_copy = remote(lam_own, lam_in, lam_sem.at[0], lam_sem.at[1], {"tp": other})
    lam_copy.start()

    loads[0].wait()
    arrived(x.at[other], x_sem.at[1])

    def norm_rows(n, carry):
        rows = pl.ds(pl.multiple_of(n * 64, 64), 64)
        first, second = x[0, rows, :].astype(F32), x[1, rows, :].astype(F32)
        squares = jnp.sum(first * first, axis=1, keepdims=True) + jnp.sum(
            second * second, axis=1, keepdims=True
        )
        scale = lax.rsqrt(squares / D + EPS)
        normed[rows, 0:1024] = (first * scale * in_gain[:, 0:1024]).astype(BF16)
        normed[rows, 1024:2048] = (second * scale * in_gain[:, 1024:2048]).astype(BF16)
        return carry

    lax.fori_loop(0, 8, norm_rows, 0)

    wo_copies = [
        remote(out_ssm, wo.at[c, 1], wo_sem.at[0], wo_sem.at[1], {"tp": other}),
        remote(out_attn, wo.at[c, 0], wo_sem.at[2], wo_sem.at[3], {"tp": other}),
    ]

    def exchange(src, dst, send, recv, j):
        to, r = 2 * c + j // 2, j % 2
        mine = jnp.logical_and(to == z, c == r)

        @pl.when(mine)
        def _():
            pltpu.make_async_copy(src.at[j], dst, recv.at[z]).start()

        @pl.when(jnp.logical_not(mine))
        def _():
            remote(src.at[j], dst, send.at[j], recv.at[z], {"sp_0": to, "tp": r}).start()

    loads[1].wait()
    loads[2].wait()
    for i in range(2):
        lanes = slice(i * PAIR, (i + 1) * PAIR)
        keys = matmul(normed[...], wk[:, lanes])
        for r in range(2):
            kv_in[2 * i + r, 0] = keys[r * HALF : (r + 1) * HALF].astype(BF16)
        values = matmul(normed[...], wv[:, lanes])
        for r in range(2):
            kv_in[2 * i + r, 1] = values[r * HALF : (r + 1) * HALF].T.astype(BF16)
        for r in range(2):
            exchange(kv_in, kv.at[0, z], zs_send, zs_recv, 2 * i + r)
    for copy in wo_copies:
        copy.start()
    def to_neighbour(slot, zz, new_slot, yy, k):
        return remote(
            kv.at[slot, zz],
            kv.at[new_slot, zz],
            ring_send.at[k],
            kv_recv.at[new_slot, zz],
            {"sp_1": yy},
        )

    def to_partner(slot, zz):
        return remote(
            kv.at[slot, zz],
            kv.at[slot + 1, zz],
            core_send.at[slot // 2, zz],
            kv_recv.at[slot + 1, zz],
            {"tp": other},
        )

    at = [z, lax.rem(z + 1, 2), jnp.where(z < 2, 2, z - 2), jnp.where(z == 3, 2, 3)]

    def serve(t):
        arrived(kv.at[0, at[t]], zs_recv.at[at[t]])
        to_neighbour(0, at[t], 6, right, t).start()
        to_neighbour(0, at[t], 2, left, 4 + t).start()
        to_partner(0, at[t]).start()

    loads[3].wait()
    for i in range(2):
        if i:
            serve(0)
        queries = matmul(normed[...], wq[:, i * PAIR : (i + 1) * PAIR])
        for r in range(2):
            q_in[2 * i + r] = queries[r * HALF : (r + 1) * HALF].T.astype(BF16)
            exchange(q_in, q.at[z], zq_send, zq_recv, 2 * i + r)


    for k in (4, 5, 6):
        loads[k].wait()
    for wide, lanes, at_lane in (
        (wx, slice(0, 256), 0),
        (wx, slice(256, 512), 256),
        (wb, slice(0, 256), 512),
        (wc, slice(0, 256), 768),
    ):
        part = matmul(normed[...], wide[:, lanes]).astype(BF16)
        pre[8:520, at_lane : at_lane + 256] = part.astype(F32)
        halo_out[:, at_lane : at_lane + 256] = part[496:512]
    halo_copy = remote(
        halo_out, halo_in, halo_sem.at[0], halo_sem.at[1], {"sp_0": next_z, "sp_1": right}
    )
    halo_copy.start()
    loads[7].wait()
    for i in range(2):
        lanes = slice(i * 256, (i + 1) * 256)
        gate[:, lanes] = matmul(normed[...], wg[:, lanes]).astype(BF16)
    loads[8].wait()
    narrow[...] = contract(ws[...], normed[...], 1, 1).astype(BF16).astype(F32)

    def convolve(blocks):
        for at_lane, (taps, lanes) in enumerate(
            (
                (conv_inner, slice(0, 256)),
                (conv_inner, slice(256, 512)),
                (conv_bvec, slice(0, 256)),
                (conv_cvec, slice(0, 256)),
            )
        ):
            here = slice(at_lane * 256, at_lane * 256 + 256)
            weight = taps[:, lanes].astype(F32)
            for n in blocks:
                first = 5 + n * BLOCK
                summed = pre[first : first + BLOCK, here] * weight[0:1]
                for o in range(1, 4):
                    summed = summed + pre[first + o : first + o + BLOCK, here] * weight[o : o + 1]
                act[n * BLOCK : (n + 1) * BLOCK, here] = (
                    summed * jax.nn.sigmoid(summed)
                ).astype(BF16)

    convolve((1, 2, 3))
    arrived(halo_in, halo_sem.at[1])
    begins = jnp.logical_and(z == 0, y == 0)
    pre[0:8, :] = halo_in[...].astype(F32)[8:16] * jnp.where(begins, 0.0, 1.0)
    convolve((0,))

    rate = jnp.zeros((8, 128), F32)
    sub = lax.broadcasted_iota(jnp.int32, (8, 128), 0)
    lane8 = lax.broadcasted_iota(jnp.int32, (8, 128), 1)
    for h in range(8):
        rate = jnp.where(sub == h, a_log[0, h], rate)
    rate = -jnp.exp(rate)
    t_at = lax.broadcasted_iota(jnp.int32, (BLOCK, BLOCK), 0)
    s_at = lax.broadcasted_iota(jnp.int32, (BLOCK, BLOCK), 1)
    causal = s_at <= t_at
    low_lane = s_at < SSM_P
    quarter = lax.broadcasted_iota(jnp.int32, (BLOCK, 256), 1) // SSM_P

    def spread(tile, first):
        pairs = [
            jnp.where(low_lane, tile[:, first + a : first + a + 1], tile[:, first + a + 1 : first + a + 2])
            for a in (0, 2)
        ]
        return jnp.concatenate(pairs, axis=1)

    def by_head(tile):
        return jnp.concatenate(
            [jnp.broadcast_to(tile[h : h + 1], (SSM_P, 128)) for h in range(tile.shape[0])], axis=0
        )

    def split_dot(left_side, right_side):
        high = right_side.astype(BF16)
        low = (right_side - high.astype(F32)).astype(BF16)
        return contract(left_side, high, 1, 1) + contract(left_side, low, 1, 1)

    state[...] = jnp.zeros_like(state)
    preceding = jnp.zeros((8, 128), F32)
    for n in range(4):
        rows = slice(n * BLOCK, (n + 1) * BLOCK)
        step_pre = narrow[:, rows]
        decay_row = decay_add[:, rows]
        size = jnp.maximum(step_pre, 0.0) + jnp.log1p(jnp.exp(-jnp.abs(step_pre)))
        running = rate * size + decay_row
        for shift in (1, 2, 4, 8, 16, 32, 64):
            running = running + jnp.where(lane8 >= shift, pltpu.roll(running, shift, 1), 0.0)
        last = jnp.broadcast_to(running[:, 127:128], (8, 128))
        to_end = jnp.exp(last - running) * size
        tall = jnp.concatenate(
            [running, to_end, jnp.exp(running), jnp.exp(running + preceding), jnp.zeros((96, 128), F32)],
            axis=0,
        ).T
        cols[rows, :] = tall
        keep = jnp.exp(last)
        preceding = preceding + last
        for g in range(2):
            lanes = slice(g * 256, (g + 1) * 256)
            inputs_x = act[rows, lanes]
            inputs_b = act[rows, 512 + g * 128 : 640 + g * 128]
            inputs_c = act[rows, 768 + g * 128 : 896 + g * 128]
            crossing = contract(inputs_c, inputs_b, 1, 1)
            mixes, own_x = [], []
            for a in range(4):
                h = 4 * g + a
                fade = jnp.exp(
                    jnp.where(causal, tall[:, h : h + 1] - running[h : h + 1, :], NEG)
                )
                mixes.append((crossing * fade * size[h : h + 1, :]).astype(BF16))
                own_x.append(jnp.where(quarter == a, inputs_x, jnp.zeros_like(inputs_x)))
            inside = matmul(jnp.concatenate(mixes, axis=1), jnp.concatenate(own_x, axis=0))
            weighted = (inputs_x.astype(F32) * spread(tall, 8 + 4 * g)).astype(BF16)
            fresh = contract(weighted, inputs_b, 0, 0)
            before = state[lanes, :]
            carried = split_dot(inputs_c, before) * spread(tall, 16 + 4 * g)
            ysum[rows, lanes] = inside + carried
            state[lanes, :] = before * by_head(keep[4 * g : 4 * g + 4]) + fresh
        if n == 0:
            serve(1)
    for j in range(4):
        st_out[j] = state[j * 128 : (j + 1) * 128, :].astype(BF16)
        tot_out[j] = jnp.concatenate(
            [jnp.broadcast_to(preceding[2 * j + e : 2 * j + e + 1], (4, 128)) for e in range(2)], axis=0
        )
    st_y[y] = st_out[y]
    tot_y[y] = tot_out[y]
    for dy in range(1, 4):
        yy = lax.rem(y + dy, 4)
        remote(st_out.at[yy], st_y.at[y], sty_send.at[0, yy], sty_recv.at[0, y], {"sp_1": yy}).start()
        remote(tot_out.at[yy], tot_y.at[y], sty_send.at[1, yy], sty_recv.at[1, y], {"sp_1": yy}).start()

    serve(2)
    serve(3)

    def wait_chunk(slot, zz):
        arrived(kv.at[slot, zz], kv_recv.at[slot, zz])

    def unit(zqs, pair, zc, masked):
        parts = []
        for zq in zqs:
            for m in range(2):
                lanes = slice(m * QK_DIM, (m + 1) * QK_DIM)
                queries = q[zq, lanes, :]
                scores = [matmul(kv[2 * pair + e, zc, 0, :, lanes], queries) for e in range(2)]
                if masked:
                    key_at = lax.broadcasted_iota(jnp.int32, scores[0].shape, 0)
                    query_at = lax.broadcasted_iota(jnp.int32, scores[0].shape, 1)
                    scores = [
                        jnp.where(key_at <= query_at, scores[0], NEG),
                        jnp.where(key_at <= query_at + (2 * c - 1) * HALF, scores[1], NEG),
                    ]
                parts.append((zq, m, scores, peak[zq, m], total[zq, m]))
        ready = []
        for zq, m, scores, old, sums in parts:
            top = jnp.maximum(
                jnp.max(scores[0], axis=0, keepdims=True), jnp.max(scores[1], axis=0, keepdims=True)
            )
            new = jnp.maximum(old, top * SCALE2)
            weights = [jnp.exp2(part * SCALE2 - new[0:1]) for part in scores]
            shrink = jnp.exp2(old - new)
            sums = sums * shrink + (
                jnp.sum(weights[0], axis=0, keepdims=True) + jnp.sum(weights[1], axis=0, keepdims=True)
            )
            value = matmul(kv[2 * pair, zc, 1], weights[0].astype(BF16)) + matmul(
                kv[2 * pair + 1, zc, 1], weights[1].astype(BF16)
            )
            ready.append((zq, m, new, sums, acc[zq, m] * shrink[0:1] + value))
        for zq, m, new, sums, value in ready:
            peak[zq, m] = new
            total[zq, m] = sums
            acc[zq, m] = value

    def over(pair, zc, low):
        def two(k, carry):
            unit([3 - 2 * k, 2 - 2 * k], pair, zc, False)
            return carry

        lax.fori_loop(0, (4 - low) // 2, two, 0)

        @pl.when(lax.rem(low, 2) == 1)
        def _():
            unit([low], pair, zc, False)
    def two_heads(tile):
        tile = jnp.exp(tile)
        return jnp.concatenate(
            [jnp.broadcast_to(tile[4 * e : 4 * e + 1], (SSM_P, 128)) for e in range(2)], axis=0
        )

    def take(t):
        wait_chunk(6, at[t])
        if t < 2:
            to_neighbour(6, at[t], 4, right, 8 + t).start()
        to_partner(6, at[t]).start()
        wait_chunk(2, at[t])
        if t >= 2:
            to_neighbour(2, at[t], 4, left, 8 + t).start()
        to_partner(2, at[t]).start()

    take(0)
    arrived(q.at[z], zq_recv.at[z])
    wait_chunk(1, z)
    unit([z], 0, z, True)
    for t in range(1, 4):
        arrived(q.at[at[t]], zq_recv.at[at[t]])

    def own_chunk(t, carry):
        zc = jnp.where(t == 0, at[0], jnp.where(t == 1, at[1], jnp.where(t == 2, at[2], at[3])))
        @pl.when(t > 0)
        def _():
            wait_chunk(1, zc)
            unit([zc], 0, zc, True)

        over(0, zc, zc + 1)
        return carry

    lax.fori_loop(0, 4, own_chunk, 0)

    def row_prefix():
        for dy in range(1, 4):
            yy = lax.rem(y + dy, 4)
            arrived(st_y.at[yy], sty_recv.at[0, yy])
            arrived(tot_y.at[yy], sty_recv.at[1, yy])
        run_s, run_t = jnp.zeros((128, 128), F32), jnp.zeros((8, 128), F32)
        for k in range(4):
            pre_s[k] = run_s
            pre_t[k] = run_t
            run_s = run_s * two_heads(tot_y[k]) + st_y[k].astype(F32)
            run_t = run_t + tot_y[k]
        row_out[...] = run_s.astype(BF16)
        rtot_out[...] = run_t
        st_z[z] = run_s.astype(BF16)
        tot_z[z] = run_t
        for dz in range(1, 4):
            where = {"sp_0": lax.rem(z + dz, 4)}
            remote(row_out, st_z.at[z], stz_send.at[0, dz], stz_recv.at[0, z], where).start()
            remote(rtot_out, tot_z.at[z], stz_send.at[1, dz], stz_recv.at[1, z], where).start()

    def far_prefix():
        for dz in range(1, 4):
            zz = lax.rem(z + dz, 4)
            arrived(st_z.at[zz], stz_recv.at[0, zz])
            arrived(tot_z.at[zz], stz_recv.at[1, zz])
        run = jnp.zeros((128, 128), F32)
        for k in range(3):
            run = jnp.where(k < z, run * two_heads(tot_z[k]) + st_z[k].astype(F32), run)
        for k in range(4):
            inc_out[k] = (run * two_heads(pre_t[k]) + pre_s[k]).astype(BF16)
        inc_in[y] = inc_out[y]
        for dy in range(1, 4):
            yy = lax.rem(y + dy, 4)
            remote(inc_out.at[yy], inc_in.at[y], inc_send.at[yy], inc_recv.at[y], {"sp_1": yy}).start()

    def finish_ssm():
        for dy in range(1, 4):
            yy = lax.rem(y + dy, 4)
            arrived(inc_in.at[yy], inc_recv.at[yy])
        came = [jnp.concatenate([inc_in[2 * g], inc_in[2 * g + 1]], axis=0) for g in range(2)]
        for n in range(4):
            rows = slice(n * BLOCK, (n + 1) * BLOCK)
            for g in range(2):
                lanes = slice(g * 256, (g + 1) * 256)
                inputs_c = act[rows, 768 + g * 128 : 896 + g * 128]
                value = ysum[rows, lanes] + contract(inputs_c, came[g], 1, 1) * spread(
                    cols[rows, :], 24 + 4 * g
                )
                opened = gate[rows, lanes].astype(F32)
                value = value * (opened * jax.nn.sigmoid(opened))
                scale = lax.rsqrt(jnp.mean(value * value, axis=1, keepdims=True) + EPS)
                ssm_all[n // 2, (n % 2) * BLOCK : (n % 2 + 1) * BLOCK, lanes] = (
                    value * scale * ssm_gain[:, lanes]
                ).astype(BF16)
        ssm_buf[c] = ssm_all[c]
        remote(ssm_all.at[other], ssm_buf.at[c], ssm_sem.at[0], ssm_sem.at[1], {"tp": other}).start()

    def project_ssm():
        arrived(ssm_buf.at[other], ssm_sem.at[1])
        loads[9].wait()
        arrived(wo.at[other, 1], wo_sem.at[1])
        for k in range(4):
            lanes = slice(k * 512, (k + 1) * 512)
            joined[:, lanes] = matmul(ssm_buf[0], wo[0, 1, :, lanes]) + matmul(
                ssm_buf[1], wo[1, 1, :, lanes]
            )

    def finish(zq, carry):
        differ = acc[zq, 0] / total[zq, 0, 0:1] - lam * (acc[zq, 1] / total[zq, 1, 0:1])
        scale = lax.rsqrt(jnp.mean(differ * differ, axis=0, keepdims=True) + EPS)
        done_out[zq] = (differ * scale * gain_col[...]).astype(BF16)

        @pl.when(zq == z)
        def _():
            pltpu.make_async_copy(done_out.at[zq], back.at[z], back_recv.at[z]).start()

        @pl.when(zq != z)
        def _():
            remote(
                done_out.at[zq], back.at[z], back_send.at[zq], back_recv.at[z], {"sp_0": zq}
            ).start()

        return carry

    def later(pair, zc):
        return zc + jnp.where(lax.rem(y + pair, 4) > y, 1, 0)

    def near(t):
        def side(k, carry):
            pair = 3 - 2 * k
            wait_chunk(2 * pair + 1, at[t])
            over(pair, at[t], later(pair, at[t]))
            return carry

        lax.fori_loop(0, 2, side, 0)

    def take_far(t):
        wait_chunk(4, at[t])
        to_partner(4, at[t]).start()

    def far(t):
        wait_chunk(5, at[t])
        over(2, at[t], later(2, at[t]))

    row_prefix()
    take(1)
    near(0)
    take(2)
    far_prefix()
    near(1)
    take(3)
    near(2)
    take_far(0)
    near(3)
    far(0)
    take_far(1)
    finish_ssm()
    take_far(2)
    far(1)
    arrived(lam_in, lam_sem.at[1])
    held = jnp.where(z // 2 == c, lam_own[lax.rem(z, 2)], lam_in[lax.rem(z, 2)])
    lam = jnp.concatenate([held, held], axis=1)[0:1]
    gain_col[...] = jnp.broadcast_to(head_gain[...], (PAIR, PAIR)).T
    whole = jnp.where(z < 2, 2, z - 2)
    lax.fori_loop(0, whole, finish, 0)
    far(2)
    take_far(3)
    lax.fori_loop(whole, at[3], finish, 0)
    project_ssm()
    far(3)
    lax.fori_loop(at[3], 4, finish, 0)
    out_copies = []
    loads[10].wait()
    arrived(wo.at[other, 0], wo_sem.at[3])
    for k, h in enumerate((z, lax.rem(z + 3, 4), lax.rem(z + 1, 4), lax.rem(z + 2, 4))):
        arrived(back.at[h], back_recv.at[h])
        weight = wo.at[h // 2, 0, pl.ds(pl.multiple_of(lax.rem(h, 2) * PAIR, PAIR), PAIR)]
        for n in range(4):
            lanes = slice(n * 512, (n + 1) * 512)
            sum_n = joined[:, lanes] + contract(back[h], weight[:, lanes], 0, 0)
            if k < 3:
                joined[:, lanes] = sum_n
            else:
                result[:, lanes] = sum_n.astype(BF16)
                out_copies.append(
                    pltpu.make_async_copy(
                        result.at[:, lanes], out_ref.at[:, lanes], out_sem.at[n]
                    )
                )
                out_copies[-1].start()

    x_copy.wait_send()
    lam_copy.wait_send()
    halo_copy.wait_send()
    for copy in wo_copies:
        copy.wait_send()
    for j in range(4):
        mine = jnp.logical_and(2 * c + j // 2 == z, c == j % 2)

        @pl.when(jnp.logical_not(mine))
        def _():
            arrived(kv_in.at[j], zs_send.at[j])
            arrived(q_in.at[j], zq_send.at[j])

    for k in range(12):
        arrived(kv.at[0, 0], ring_send.at[k])
    for s in range(4):
        for t in range(4):
            arrived(kv.at[0, 0], core_send.at[s, t])
    for d in range(1, 4):
        yy = lax.rem(y + d, 4)
        arrived(st_out.at[yy], sty_send.at[0, yy])
        arrived(tot_out.at[yy], sty_send.at[1, yy])
        arrived(inc_out.at[yy], inc_send.at[yy])
        arrived(row_out, stz_send.at[0, d])
        arrived(rtot_out, stz_send.at[1, d])
    arrived(ssm_all.at[0], ssm_sem.at[0])
    for d in range(1, 4):
        arrived(done_out.at[0], back_send.at[lax.rem(z + d, 4)])
    for copy in out_copies:
        copy.wait()


def per_device(
    hidden_in,
    in_gain,
    w_query,
    w_key,
    w_value,
    w_gate,
    w_inner,
    w_bvec,
    w_cvec,
    w_step,
    conv_inner,
    conv_bvec,
    conv_cvec,
    a_log,
    decay_add,
    lambdas,
    head_gain,
    ssm_gain,
    out_attn,
    out_ssm,
):
    vmem = pl.BlockSpec(memory_space=pltpu.VMEM)
    smem = pl.BlockSpec(memory_space=pltpu.SMEM)
    away = pl.BlockSpec(memory_space=pl.ANY)
    dma = pltpu.SemaphoreType.DMA
    buf = pltpu.VMEM
    return pl.pallas_call(
        layer_kernel,
        out_shape=jax.ShapeDtypeStruct((HALF, D), BF16),
        in_specs=[away, vmem]
        + [away] * 8
        + [vmem] * 3
        + [smem, vmem, smem, vmem, vmem, away, away],
        out_specs=away,
        scratch_shapes=[
            buf((2, ROWS, 1024), BF16),
            buf((ROWS, D), BF16),
            buf((D, 512), BF16),
            buf((D, 512), BF16),
            buf((D, 512), BF16),
            buf((D, 512), BF16),
            buf((D, 512), BF16),
            buf((D, 256), BF16),
            buf((D, 256), BF16),
            buf((8, D), BF16),
            buf((2, 2, 512, D), BF16),
            buf((4, 2, HALF, PAIR), BF16),
            buf((4, PAIR, HALF), BF16),
            buf((8, 4, 2, HALF, PAIR), BF16),
            buf((4, PAIR, HALF), BF16),
            buf((4, 2, PAIR, HALF), F32),
            buf((4, 2, 8, HALF), F32),
            buf((4, 2, 8, HALF), F32),
            buf((4, PAIR, HALF), BF16),
            buf((4, PAIR, HALF), BF16),
            buf((520, 1024), F32),
            buf((16, 1024), BF16),
            buf((16, 1024), BF16),
            buf((ROWS, 1024), BF16),
            buf((ROWS, 512), BF16),
            buf((8, ROWS), F32),
            buf((ROWS, 128), F32),
            buf((ROWS, 512), F32),
            buf((512, 128), F32),
            buf((4, 128, 128), BF16),
            buf((4, 8, 128), F32),
            buf((4, 128, 128), BF16),
            buf((4, 8, 128), F32),
            buf((128, 128), BF16),
            buf((8, 128), F32),
            buf((4, 128, 128), BF16),
            buf((4, 8, 128), F32),
            buf((4, 128, 128), F32),
            buf((4, 8, 128), F32),
            buf((4, 128, 128), BF16),
            buf((4, 128, 128), BF16),
            buf((2, HALF, 512), BF16),
            buf((2, HALF, 512), BF16),
            buf((HALF, D), F32),
            buf((2, 8, 128), F32),
            buf((2, 8, 128), F32),
            buf((PAIR, PAIR), F32),
            buf((HALF, D), BF16),
            dma((11,)),
            dma((2,)),
            dma((4,)),
            dma((4,)),
            dma((4,)),
            dma((4,)),
            dma((4,)),
            dma((12,)),
            dma((8, 4)),
            dma((4, 4)),
            dma((4,)),
            dma((4,)),
            dma((2,)),
            dma((2, 4)),
            dma((2, 4)),
            dma((2, 4)),
            dma((2, 4)),
            dma((2,)),
            dma((2,)),
            dma((4,)),
            dma((4,)),
            dma((4,)),
        ],
        compiler_params=pltpu.CompilerParams(
            collective_id=0, has_side_effects=True, vmem_limit_bytes=63 * 2**20
        ),
    )(
        hidden_in,
        in_gain.reshape(1, D),
        w_query,
        w_key,
        w_value,
        w_gate,
        w_inner,
        w_bvec,
        w_cvec,
        w_step.T,
        conv_inner,
        conv_bvec,
        conv_cvec,
        a_log.reshape(1, 8),
        decay_add.T,
        lambdas.reshape(1, 2),
        head_gain.reshape(1, PAIR),
        ssm_gain.reshape(1, 512),
        out_attn,
        out_ssm,
    )


def solution(mesh):
    split = Mesh(
        mesh.devices.reshape(4, 4, mesh.shape["fs"], mesh.shape["tp"]), ("sp_0", "sp_1", "fs", "tp")
    )
    in_specs = (
        P(FS_SP, "tp"),
        P(),
        P(None, "tp"),
        P(None, "tp"),
        P(None, "tp"),
        P(None, "tp"),
        P(None, "tp"),
        P(None, "tp"),
        P(None, "tp"),
        P(None, "tp"),
        P(None, "tp"),
        P(None, "tp"),
        P(None, "tp"),
        P("tp"),
        P(FS_SP, "tp"),
        P("tp"),
        P(),
        P("tp"),
        P("tp", None),
        P("tp", None),
    )
    out_specs = P(FS_SP_TP, None)
    return jax.shard_map(
        per_device, mesh=split, in_specs=in_specs, out_specs=out_specs, check_vma=False
    )
```
